128 devices in a mesh: grp: 4 (over y, x), ep: 32 (over z, core).
Axes of the slice: x: 2, y: 2, z: 16, core: 2. Of those that a mesh axis runs over, the one named last changes fastest.
The devices are a block of a 8x8x16 slice.
Arguments:
- tokens_in: bfloat16 [256, 4096], P(('grp', 'ep')), parts along dimension 0, may hold values from -6 to 6
- mix_gain: float32 [4096], replicated, may hold values from 0.1 to 1.9
- w_gate_z: bfloat16 [4096, 4096], P(None, 'ep'), may hold values from -0.09375 to 0.09375
- w_value: bfloat16 [4096, 4096], P(None, 'ep'), may hold values from -0.09375 to 0.09375
- w_in_bc: bfloat16 [4096, 1024], P(None, 'ep'), may hold values from -0.09375 to 0.09375
- w_step: bfloat16 [4096, 64], replicated, may hold values from -0.09375 to 0.09375
- step_bias: float32 [64], replicated, may hold values from -4 to 0.5
- decay_log: float32 [64], replicated, may hold values from -1.5 to 2
- skip_gain: float32 [64], replicated, may hold values from 0.3 to 1.7
- conv_x_weight: float32 [4, 4096], replicated, may hold values from -3 to 3
- conv_bc_weight: float32 [4, 1024], replicated, may hold values from -3 to 3
- conv_x_state: bfloat16 [256, 3, 4096], P(('grp', 'ep')), parts along dimension 0, may hold values from -6 to 6
- conv_bc_state: bfloat16 [256, 3, 1024], P(('grp', 'ep')), parts along dimension 0, may hold values from -6 to 6
- ssm_state: float32 [256, 64, 64, 128], P(('grp', 'ep')), parts along dimension 0, may hold values from -3 to 3
- inner_gain: float32 [4096], replicated, may hold values from 0.1 to 1.9
- out_weight: bfloat16 [4096, 4096], P(None, 'ep'), may hold values from -0.09375 to 0.09375
- ffn_gain: float32 [4096], replicated, may hold values from 0.1 to 1.9
- expert_gate: bfloat16 [32, 4096, 512], P('ep'), may hold values from -0.09375 to 0.09375
- expert_up: bfloat16 [32, 4096, 512], P('ep'), may hold values from -0.09375 to 0.09375
- expert_down: bfloat16 [32, 512, 4096], P('ep'), may hold values from -0.25 to 0.25
- routes: int32 [256, 4], P(('grp', 'ep')), parts along dimension 0, may hold values from 0 to 31, all different within a row; in each aligned block of 2 rows (0 to 1, 2 to 3, ...) at most 2 rows name the same one
- route_weight: float32 [256, 4], P(('grp', 'ep')), parts along dimension 0, may hold values from 0.1 to 1
Outputs:
- out_tokens: bfloat16 [256, 4096], P(('grp', 'ep')), parts along dimension 0
- new_state: float32 [256, 64, 64, 128], P(('grp', 'ep')), parts along dimension 0
- new_conv_x: bfloat16 [256, 3, 4096], P(('grp', 'ep')), parts along dimension 0
- new_conv_bc: bfloat16 [256, 3, 1024], P(('grp', 'ep')), parts along dimension 0
The draws below stay inside these ranges and needn't reach their ends.
There are 4 independent parts, one for each index of `grp`. The reference program is written for one: setup_inputs(seed, part) draws one part's arguments, and reference() takes and returns one part's arrays. A program takes and returns all parts, laid end to end along the dimension named above; an argument that names none is the same for every part. Nothing has to cross between parts.
Inputs may be any that keep to these rules, and one draw needn't show every extreme that they name: `routes`: each row names 4 different experts. Among the rows of one device no expert is named more than 2 times, and some device names some expert exactly 2 times.
All inputs are finite; a program needn't handle non-finite values.
Results may differ from the reference program's by a relative error of at most 0.015.
Values may be sent and summed in bfloat16 or wider, within the bound.
A program may use at most 64 MiB of HBM per device.

```python
import math
import jax
import jax.numpy as jnp
import numpy as np
from jax import lax

D = 4096
HEADS = 64
HEAD_DIM = 64
GROUPS = 4
NSTATE = 128
CONV = 4
FF = 512
TOPK = 4
SLOT = 2
SEQ_DEV = 2
INNER = 4096
EXPERTS = 32
BATCH = 64


def block_levels(key, dims, shards, least, high):
    level, own = 1.0, jax.random.fold_in(key, 6)
    for position, blocks in shards:
        heights = jnp.exp(jax.random.uniform(jax.random.fold_in(own, position), (blocks,), jnp.float32, least / len(shards), high / len(shards)))
        level = level * jnp.repeat(heights, dims[position] // blocks).reshape([-1 if axis == position else 1 for axis in range(len(dims))])
    return level


def assign_block(rng, own, number, rows, amount, top, bound, lean):
    sequence = jax.random.permutation(rng, amount)
    crowded, common = shares(amount, rows * top, bound, lean, True), shares(amount, rows * top, bound, lean, False)
    places = jnp.arange(amount)

    def named(sizes, rotation):
        used = int((sizes > 0).sum())
        fixed = max(1, used // 4)
        shifted = fixed + (places - fixed + rotation * (used - fixed)) % max(1, amount - fixed)
        return jnp.zeros((amount,), jnp.int32).at[sequence[jnp.where(places < fixed, places, shifted)]].set(jnp.asarray(sizes, jnp.int32))

    sizes = jnp.where(number % 4 == 0, named(crowded, number // 4), named(common, number - number // 4 - 1))
    mixed = jax.random.permutation(jax.random.fold_in(own, 3), amount)
    donor, receiver = mixed[0:amount // 2 * 2:2], mixed[1:amount // 2 * 2:2]
    margin = jnp.minimum(sizes[donor] - 1, bound - sizes[receiver]) // 2
    margin = jnp.where((donor == sequence[0]) | (receiver == sequence[0]) | (sizes[receiver] == 0), 0, jnp.maximum(margin, 0))
    shifted = jax.random.randint(jax.random.fold_in(own, 4), (amount // 2,), 0, 1 << 20) % (margin + 1)
    sizes = sizes.at[donor].add(-shifted).at[receiver].add(shifted)
    members = jnp.searchsorted(jnp.cumsum(sizes), jnp.arange(rows * top), side="right").astype(jnp.int32)
    table = members.reshape(top, rows).T
    table = table[jax.random.permutation(jax.random.fold_in(own, 1), rows)]
    rotation = jax.random.randint(jax.random.fold_in(own, 2), (rows, 1), 0, top)
    return jnp.take_along_axis(table, (jnp.arange(top)[None, :] + rotation) % top, axis=1)


def shares(amount, total, bound, lean, full):
    loads = [(1 << 20) // math.isqrt(rank ** lean) + 1 for rank in range(1, amount + 1)]
    largest = bound if full else min(bound, max(-(-total // amount), total * loads[0] // sum(loads)))
    least = 1 if total - largest >= amount - 1 else 0
    given, surplus = [largest] + [least] * (amount - 1), total - largest - least * (amount - 1)
    while surplus > 0:
        free = [i for i in range(1, amount) if given[i] < largest] or [i for i in range(1, amount) if given[i] < bound]
        pool, remaining = sum([loads[i] for i in free]), surplus
        for i in free:
            extra = min(bound - given[i], max(1, remaining * loads[i] // pool), surplus)
            given[i] = given[i] + extra
            surplus = surplus - extra
    return np.array(given)


def normal_values(own_key, shape, deviation, most, pieces=(), kind=jnp.bfloat16):
    array = jax.random.normal(own_key, shape, jnp.float32) * deviation
    if len(pieces) > 0:
        array = block_levels(own_key, shape, pieces, -0.22, 0.18) * array
    return jnp.clip(array, min=-most, max=most).astype(kind)


def setup_inputs(seed: int = 0, part: int = 0) -> dict:
    key_of = jax.random.split(jax.random.key(seed), 23)
    own_keys = jax.random.split(jax.random.fold_in(key_of[22], part), 23)
    tokens_in = normal_values(own_keys[0], (BATCH, D), 1.0, 6.0, ((0, 32),))
    mix_gain = jnp.clip(1.0 + 0.18 * jax.random.normal(key_of[1], (D,), jnp.float32), 0.1, 1.9)
    w_gate_z = normal_values(key_of[2], (D, INNER), D ** -0.5, 0.09375, ((1, 32),))
    w_value = normal_values(key_of[3], (D, INNER), D ** -0.5, 0.09375, ((1, 32),))
    w_in_bc = normal_values(key_of[4], (D, 2 * GROUPS * NSTATE), D ** -0.5, 0.09375, ((1, 32),))
    w_step = normal_values(key_of[5], (D, HEADS), D ** -0.5, 0.09375)
    step_bias = jnp.clip(jax.random.uniform(key_of[6], (HEADS,), jnp.float32, -4.0, 0.5), -4.0, 0.5)
    decay_log = jnp.clip(jax.random.uniform(key_of[7], (HEADS,), jnp.float32, -1.5, 2.0), -1.5, 2.0)
    skip_gain = jnp.clip(jax.random.uniform(key_of[8], (HEADS,), jnp.float32, 0.3, 1.7), 0.3, 1.7)
    conv_x_weight = normal_values(key_of[9], (CONV, INNER), 0.5, 3.0, (), jnp.float32)
    conv_bc_weight = normal_values(key_of[10], (CONV, 2 * GROUPS * NSTATE), 0.5, 3.0, (), jnp.float32)
    conv_x_state = normal_values(own_keys[11], (BATCH, CONV - 1, INNER), 1.0, 6.0, ((0, 32),))
    conv_bc_state = normal_values(own_keys[12], (BATCH, CONV - 1, 2 * GROUPS * NSTATE), 1.0, 6.0, ((0, 32),))
    ssm_state = normal_values(own_keys[13], (BATCH, HEADS, HEAD_DIM, NSTATE), 0.3, 3.0, ((0, 32),), jnp.float32)
    inner_gain = jnp.clip(1.0 + 0.18 * jax.random.normal(key_of[14], (INNER,), jnp.float32), 0.1, 1.9)
    out_weight = normal_values(key_of[15], (INNER, D), INNER ** -0.5, 0.09375, ((1, 32),))
    ffn_gain = jnp.clip(1.0 + 0.18 * jax.random.normal(key_of[16], (D,), jnp.float32), 0.1, 1.9)
    expert_gate = normal_values(key_of[17], (EXPERTS, D, FF), D ** -0.5, 0.09375, ((0, 32),))
    expert_up = normal_values(key_of[18], (EXPERTS, D, FF), D ** -0.5, 0.09375, ((0, 32),))
    expert_down = normal_values(key_of[19], (EXPERTS, FF, D), FF ** -0.5, 0.25, ((0, 32),))
    routes_keys = jax.random.split(jax.random.fold_in(own_keys[20], 1), BATCH // SEQ_DEV)
    routes_turns = jax.random.permutation(jax.random.fold_in(own_keys[20], 3), BATCH // SEQ_DEV)
    routes = jax.vmap(lambda own, number: assign_block(jax.random.fold_in(own_keys[20], 2), own, number, SEQ_DEV, EXPERTS, TOPK, SLOT, 2))(routes_keys, routes_turns).reshape((BATCH, TOPK))
    route_weight = jnp.clip(0.1 + 0.9 * jax.random.uniform(own_keys[21], (BATCH, TOPK), jnp.float32) ** block_levels(own_keys[21], (BATCH, TOPK), ((0, 32),), -0.2, 0.2), 0.1, 1.0)
    return dict(tokens_in=tokens_in, mix_gain=mix_gain, w_gate_z=w_gate_z, w_value=w_value, w_in_bc=w_in_bc, w_step=w_step, step_bias=step_bias, decay_log=decay_log, skip_gain=skip_gain, conv_x_weight=conv_x_weight, conv_bc_weight=conv_bc_weight, conv_x_state=conv_x_state, conv_bc_state=conv_bc_state, ssm_state=ssm_state, inner_gain=inner_gain, out_weight=out_weight, ffn_gain=ffn_gain, expert_gate=expert_gate, expert_up=expert_up, expert_down=expert_down, routes=routes, route_weight=route_weight)


def rms_norm(values, gain):
    floats = values.astype(jnp.float32)
    return floats * lax.rsqrt(lax.optimization_barrier(jnp.mean(floats * floats, axis=-1, keepdims=True)) + 1e-06) * gain

def conv_step(window_state, newest, taps):
    window = jnp.concatenate([window_state, newest[:, None, :]], axis=1)
    mixed = jax.nn.silu(lax.optimization_barrier(jnp.sum(window.astype(jnp.float32) * taps[None, :, :], axis=1)))
    return (mixed, window[:, 1:])

def reference(tokens_in, mix_gain, w_gate_z, w_value, w_in_bc, w_step, step_bias, decay_log, skip_gain, conv_x_weight, conv_bc_weight, conv_x_state, conv_bc_state, ssm_state, inner_gain, out_weight, ffn_gain, expert_gate, expert_up, expert_down, routes, route_weight):
    batch_rows = tokens_in.shape[0]
    normed = rms_norm(tokens_in, mix_gain).astype(jnp.bfloat16)
    z_pre = jnp.dot(normed, w_gate_z, preferred_element_type=jnp.float32).astype(jnp.bfloat16)
    x_pre = jnp.dot(normed, w_value, preferred_element_type=jnp.float32).astype(jnp.bfloat16)
    bc_pre = jnp.dot(normed, w_in_bc, preferred_element_type=jnp.float32).astype(jnp.bfloat16)
    step_pre = jnp.dot(normed, w_step, preferred_element_type=jnp.float32)
    x_conv, new_conv_x = conv_step(conv_x_state, x_pre, conv_x_weight)
    bc_conv, new_conv_bc = conv_step(conv_bc_state, bc_pre, conv_bc_weight)
    group_cols = GROUPS * NSTATE
    in_map = jnp.repeat(bc_conv[:, :group_cols].reshape(batch_rows, GROUPS, NSTATE), HEADS // GROUPS, axis=1)
    out_map = jnp.repeat(bc_conv[:, group_cols:].reshape(batch_rows, GROUPS, NSTATE), HEADS // GROUPS, axis=1)
    step = jax.nn.softplus(step_pre + step_bias[None, :])
    decay = jnp.exp(-step * jnp.exp(decay_log)[None, :])
    x_heads = x_conv.reshape(batch_rows, HEADS, HEAD_DIM)
    new_state = decay[:, :, None, None] * ssm_state + (step[:, :, None] * x_heads)[..., None] * in_map[:, :, None, :]
    head_out = jnp.einsum('bhn,bhpn->bhp', out_map, new_state, precision=lax.Precision.HIGHEST)
    head_out = head_out + skip_gain[None, :, None] * x_heads
    gated = head_out.reshape(batch_rows, HEADS * HEAD_DIM) * jax.nn.silu(z_pre.astype(jnp.float32))
    mixed = rms_norm(gated, inner_gain).astype(jnp.bfloat16)
    mix_out = jnp.dot(mixed, out_weight, preferred_element_type=jnp.float32).astype(jnp.bfloat16)
    resid = (tokens_in.astype(jnp.float32) + mix_out.astype(jnp.float32)).astype(jnp.bfloat16)
    ffn_in = rms_norm(resid, ffn_gain).astype(jnp.bfloat16)
    n_experts = expert_gate.shape[0]
    expert_ids = jnp.arange(n_experts, dtype=jnp.int32)
    dense_weight = lax.optimization_barrier(jnp.sum((routes[:, :, None] == expert_ids[None, None, :]).astype(jnp.float32) * route_weight[:, :, None], axis=1))

    def one_expert(total, index):
        gate_part = jnp.dot(ffn_in, expert_gate[index], preferred_element_type=jnp.float32)
        up_part = jnp.dot(ffn_in, expert_up[index], preferred_element_type=jnp.float32)
        act = (jax.nn.silu(gate_part) * up_part).astype(jnp.bfloat16)
        expert_row = jnp.dot(act, expert_down[index], preferred_element_type=jnp.float32).astype(jnp.bfloat16)
        column = lax.dynamic_slice_in_dim(dense_weight, index, 1, 1)
        return (total + column * expert_row.astype(jnp.float32), None)
    summed, _ = lax.scan(one_expert, jnp.zeros(tokens_in.shape, jnp.float32), expert_ids)
    out_tokens = (resid.astype(jnp.float32) + summed).astype(jnp.bfloat16)
    return (out_tokens, new_state, new_conv_x, new_conv_bc)
```

```python
import functools

import jax
import jax.numpy as jnp
from jax import lax
from jax.experimental import pallas as pl
from jax.experimental.pallas import tpu as pltpu
from jax.sharding import PartitionSpec as P

HEADS = 64
HEAD_DIM = 64
GROUPS = 4
NSTATE = 128
TOPK = 4
GRP_EP = ("grp", "ep")
MESH = pl.DeviceIdType.MESH
F32 = jnp.float32
BF16 = jnp.bfloat16
LANES = 128
PITCH = 40

OWN = (6, -6, 3, -3, 1, -1)
RELAYS = (3, -3, 6, -6)


class Comm:
    def __init__(self, ep):
        self.ep = ep
        self.nz = ep // 2
        self.me = lax.axis_index("ep")
        self.core = lax.rem(self.me, 2)
        self.z = lax.div(self.me, 2)

    def at(self, offset, core):
        return lax.rem(self.z + offset + self.nz, self.nz) * 2 + core

    def partner(self):
        return self.z * 2 + (1 - self.core)

    def barrier(self):
        sem = pltpu.get_barrier_semaphore()

        def greet(i, carry):
            pl.semaphore_signal(
                sem, inc=1, device_id={"ep": lax.rem(self.me + i, self.ep)}, device_id_type=MESH
            )
            return carry

        lax.fori_loop(1, self.ep, greet, 0)
        return lambda: pl.semaphore_wait(sem, self.ep - 1)

    def copy(self, src, dst, send, recv, to):
        return pltpu.make_async_remote_copy(
            src_ref=src, dst_ref=dst, send_sem=send, recv_sem=recv, device_id={"ep": to}, device_id_type=MESH
        )

    def gather(self, buf, send, recv, landed):
        core, me = self.core, self.me

        def pass_on(block, to):
            self.copy(buf.at[block], buf.at[block], send, recv.at[block], to).start()

        def arrive(block):
            self.copy(buf.at[block], buf.at[block], send, recv.at[block], me).wait_recv()

        for d in OWN:
            pass_on(me, self.at(d, core))
        pass_on(me, self.partner())
        landed(me)
        extra = 2 - 4 * core
        for d in RELAYS:
            block = self.at(-d, core)
            arrive(block)
            pass_on(block, self.at(1, core))
            pass_on(block, self.at(-1, core))
            if d == 6:

                @pl.when(core == 0)
                def _(block=block):
                    pass_on(block, self.at(2, core))

            if d == -6:

                @pl.when(core == 1)
                def _(block=block):
                    pass_on(block, self.at(-2, core))

            pass_on(block, self.partner())
            landed(block)
        del extra
        for d in (1, -1, 2, -2, 4, -4, 5, -5, 7, -7, 8):
            block = self.at(-d, core)
            arrive(block)
            pass_on(block, self.partner())
            landed(block)

        def other(i, carry):
            block = self.at(i, 1 - core)
            arrive(block)
            landed(block)
            return carry

        lax.fori_loop(0, self.nz, other, 0)
        n = self.nz - 1 + self.nz
        whole = buf.at[pl.ds(0, n)]
        self.copy(whole, whole, send, recv.at[0], me).wait_send()

    def exchange(self, out, back, send, recv):
        me, ep, nz = self.me, self.ep, self.nz

        def one(to):
            self.copy(out.at[to], back.at[me], send, recv.at[me], to).start()

        def far_first(k, carry):
            offset = (nz // 2 - lax.div(k + 1, 2)) * (1 - 2 * lax.rem(k, 2))
            one(self.at(offset, 0))
            one(self.at(offset, 1))
            return carry

        lax.fori_loop(0, nz - 1, far_first, 0)
        one(self.partner())
        back[me] = out[me]

    def exchanged(self, out, back, send, recv, landed):
        me, ep = self.me, self.ep
        landed(me)

        def one(i, carry):
            frm = lax.rem(me + i, ep)
            self.copy(back.at[frm], back.at[frm], send, recv.at[frm], me).wait_recv()
            landed(frm)
            return carry

        lax.fori_loop(1, ep, one, 0)
        whole = out.at[pl.ds(0, ep - 1)]
        self.copy(whole, whole, send, recv.at[0], me).wait_send()


def tall(x, n):
    return x.reshape(n, x.shape[0] // n, x.shape[1])


def project_kernel(
    ep, tok_hbm, gain, wz_hbm, wx_hbm, wbc_hbm, wst_hbm, routes, weights,
    r_out, xraw_out, own_out,
    buf, stage, lhs, wz, wx, wbc, wst, flat, out, back,
    load, wload, gsend, grecv, xsend, xrecv,
):
    comm = Comm(ep)
    me = comm.me
    ready = comm.barrier()
    own = pltpu.make_async_copy(tok_hbm, buf.at[me], load)
    own.start()
    pulls = [
        pltpu.make_async_copy(a, b, wload.at[i])
        for i, (a, b) in enumerate(((wz_hbm, wz), (wx_hbm, wx), (wbc_hbm, wbc), (wst_hbm, wst)))
    ]
    for p in pulls:
        p.start()
    own.wait()
    ready()

    def landed(block):
        both = buf[block].astype(F32)
        for r in range(2):
            stage[pl.ds(pl.multiple_of((block * 2 + r) * PITCH, 8), 32), :] = both[r]

    comm.gather(buf, gsend, grecv, landed)
    square = jnp.zeros((64, LANES), F32)
    for j in range(32):
        x = stage[pl.ds(j, 64, stride=PITCH), :]
        square = square + x * x
        xraw_out[:, j * LANES : (j + 1) * LANES] = x.astype(BF16)
        lhs[:, j * LANES : (j + 1) * LANES] = (x * gain[j : j + 1, :]).astype(BF16)
    scale = lax.rsqrt(jnp.sum(square, axis=1, keepdims=True) / 4096.0 + 1e-6)
    for p in pulls:
        p.wait()
    left = lhs[...]
    z = jnp.dot(left, wz[...], preferred_element_type=F32) * scale
    x = jnp.dot(left, wx[...], preferred_element_type=F32) * scale
    bc = jnp.dot(left, wbc[...], preferred_element_type=F32) * scale
    st = jnp.dot(left, wst[...], preferred_element_type=F32) * scale
    lane = lax.broadcasted_iota(jnp.int32, (1, LANES), 1)
    spread = jnp.concatenate([bc, bc, bc, bc], axis=1)
    spread = jnp.where(lax.div(lane, 32) == lax.rem(me, 4), spread, 0.0)
    flat[pl.ds(0, 64, stride=4), :] = z
    flat[pl.ds(1, 64, stride=4), :] = x
    flat[pl.ds(2, 64, stride=4), :] = spread
    dense = jnp.zeros((1, LANES), F32)
    for r in range(2):
        for k in range(TOPK):
            dense = dense + jnp.where(lane == routes[r, k] + 32 * r, weights[r, k], 0.0)
    high = dense.astype(BF16).astype(F32)
    flat[pl.ds(3, 32, stride=8), :] = jnp.broadcast_to(high, (32, LANES))
    flat[pl.ds(7, 32, stride=8), :] = jnp.broadcast_to(dense - high, (32, LANES))
    out[...] = tall(flat[...], 32).astype(BF16)
    comm.exchange(out, back, xsend, xrecv)
    own_out[...] = st
    comm.exchanged(out, back, xsend, xrecv, lambda frm: None)
    r_out[...] = back[...]


def mix_kernel(
    ep, mix_hbm, xraw, r_in, gain, wo_hbm, wg_hbm, wu_hbm, wd_hbm,
    out_ref,
    buf, buf3, stage, lhs, wo, wg, wu, wd, act, flat, wide, half_out, half_in, mine, send_rows, got_rows, total,
    load, wload, gsend, grecv, gsend3, grecv3, hsend, hrecv, xsend, xrecv,
):
    comm = Comm(ep)
    me, core = comm.me, comm.core
    ready = comm.barrier()
    own = pltpu.make_async_copy(mix_hbm, buf.at[me], load)
    own.start()
    pulls = [
        pltpu.make_async_copy(a, b, wload.at[i])
        for i, (a, b) in enumerate(((wo_hbm, wo), (wg_hbm.at[0], wg), (wu_hbm.at[0], wu), (wd_hbm.at[0], wd)))
    ]
    for p in pulls:
        p.start()
    flat[...] = r_in[...].astype(F32).reshape(256, LANES)
    lane = lax.broadcasted_iota(jnp.int32, (32, LANES), 1)
    dense = flat[pl.ds(3, 32, stride=8), :] + flat[pl.ds(7, 32, stride=8), :]
    for r in range(2):
        picked = jnp.sum(jnp.where(lane == me + 32 * r, dense, 0.0), axis=1, keepdims=True)
        wide[pl.ds(r, 32, stride=2), :] = jnp.broadcast_to(picked, (32, LANES))
    own.wait()
    ready()

    def landed(block):
        both = buf[block].astype(F32)
        for r in range(2):
            stage[pl.ds(pl.multiple_of((block * 2 + r) * PITCH, 8), 32), :] = both[r]

    comm.gather(buf, gsend, grecv, landed)
    for j in range(32):
        lhs[:, j * LANES : (j + 1) * LANES] = stage[pl.ds(j, 64, stride=PITCH), :].astype(BF16)
    pulls[0].wait()
    buf3[me] = jnp.dot(lhs[...], wo[...], preferred_element_type=F32).astype(BF16)
    comm.gather(buf3, gsend3, grecv3, lambda block: None)
    square = jnp.zeros((64, LANES), F32)
    for j in range(32):
        cols = slice(j * LANES, (j + 1) * LANES)
        resid = (xraw[:, cols].astype(F32) + buf3[j].astype(F32)).astype(BF16).astype(F32)
        square = square + resid * resid
        stage[pl.ds(j, 64, stride=PITCH), :] = resid
        lhs[:, cols] = (resid * gain[j : j + 1, :]).astype(BF16)
    scale = lax.rsqrt(jnp.sum(square, axis=1, keepdims=True) / 4096.0 + 1e-6)
    pulls[1].wait()
    pulls[2].wait()
    left = lhs[...]
    g = jnp.dot(left, wg[...], preferred_element_type=F32) * scale
    u = jnp.dot(left, wu[...], preferred_element_type=F32) * scale
    act[...] = (jax.nn.silu(g) * u).astype(BF16)
    pulls[3].wait()
    weight = wide[...]

    def rows(half, k):
        cols = pl.ds(pl.multiple_of(half * 2048 + k * 512, 512), 512)
        y = jnp.dot(act[...], wd[:, cols], preferred_element_type=F32).astype(BF16).astype(F32)
        return y * jnp.concatenate([weight] * 4, axis=1)

    for k in range(4):
        half_out[:, k * 512 : (k + 1) * 512] = rows(1 - core, k).astype(BF16)
    swap = comm.copy(half_out, half_in, hsend, hrecv, comm.partner())
    swap.start()
    for k in range(4):
        mine[:, k * 512 : (k + 1) * 512] = rows(core, k)
    swap.wait()
    for j in range(16):
        cols = slice(j * LANES, (j + 1) * LANES)
        total[pl.ds(j, 64, stride=24), :] = mine[:, cols] + half_in[:, cols].astype(F32)

    def pack(t, carry):
        for r in range(2):
            send_rows[t, r] = total[pl.ds(pl.multiple_of((t * 2 + r) * 24, 8), 16), :].astype(BF16)
        return carry

    lax.fori_loop(0, ep, pack, 0)
    comm.exchange(send_rows, got_rows, xsend, xrecv)
    for r in range(2):
        total[pl.ds(r * 32, 32), :] = stage[pl.ds(pl.multiple_of((me * 2 + r) * PITCH, 8), 32), :]

    def arrived(frm):
        h = lax.rem(frm, 2)
        for r in range(2):
            at = pl.ds(pl.multiple_of(r * 32 + h * 16, 8), 16)
            total[at, :] = total[at, :] + got_rows[frm, r].astype(F32)

    comm.exchanged(send_rows, got_rows, xsend, xrecv, arrived)
    out_ref[...] = total[pl.ds(0, 64), :].astype(BF16)


def vmem():
    return pl.BlockSpec(memory_space=pltpu.VMEM)


def hbm():
    return pl.BlockSpec(memory_space=pl.ANY)


def smem():
    return pl.BlockSpec(memory_space=pltpu.SMEM)


def project(ep, tok, gain, wz, wx, wbc, wst, routes, weights):
    dma = pltpu.SemaphoreType.DMA
    return pl.pallas_call(
        functools.partial(project_kernel, ep),
        out_shape=(
            jax.ShapeDtypeStruct((ep, 8, LANES), BF16),
            jax.ShapeDtypeStruct((64, 4096), BF16),
            jax.ShapeDtypeStruct((64, 64), F32),
        ),
        in_specs=[hbm(), vmem(), hbm(), hbm(), hbm(), hbm(), smem(), smem()],
        out_specs=(vmem(), vmem(), vmem()),
        scratch_shapes=[
            pltpu.VMEM((ep, 2, 32, LANES), BF16),
            pltpu.VMEM((64 * PITCH, LANES), F32),
            pltpu.VMEM((64, 4096), BF16),
            pltpu.VMEM(wz.shape, BF16),
            pltpu.VMEM(wx.shape, BF16),
            pltpu.VMEM(wbc.shape, BF16),
            pltpu.VMEM(wst.shape, BF16),
            pltpu.VMEM((256, LANES), F32),
            pltpu.VMEM((ep, 8, LANES), BF16),
            pltpu.VMEM((ep, 8, LANES), BF16),
            dma, dma((4,)), dma, dma((ep,)), dma, dma((ep,)),
        ],
        compiler_params=pltpu.CompilerParams(collective_id=0, has_side_effects=True),
        name="project",
    )(tok, gain, wz, wx, wbc, wst, routes, weights)


def mix(ep, mixed, xraw, r, gain, wo, wg, wu, wd):
    dma = pltpu.SemaphoreType.DMA
    return pl.pallas_call(
        functools.partial(mix_kernel, ep),
        out_shape=jax.ShapeDtypeStruct((64, LANES), BF16),
        in_specs=[hbm(), vmem(), vmem(), vmem(), hbm(), hbm(), hbm(), hbm()],
        out_specs=vmem(),
        scratch_shapes=[
            pltpu.VMEM((ep, 2, 32, LANES), BF16),
            pltpu.VMEM((ep, 64, LANES), BF16),
            pltpu.VMEM((64 * PITCH, LANES), F32),
            pltpu.VMEM((64, 4096), BF16),
            pltpu.VMEM(wo.shape, BF16),
            pltpu.VMEM(wg.shape[1:], BF16),
            pltpu.VMEM(wu.shape[1:], BF16),
            pltpu.VMEM(wd.shape[1:], BF16),
            pltpu.VMEM((64, 512), BF16),
            pltpu.VMEM((256, LANES), F32),
            pltpu.VMEM((64, LANES), F32),
            pltpu.VMEM((64, 2048), BF16),
            pltpu.VMEM((64, 2048), BF16),
            pltpu.VMEM((64, 2048), F32),
            pltpu.VMEM((ep, 2, 16, LANES), BF16),
            pltpu.VMEM((ep, 2, 16, LANES), BF16),
            pltpu.VMEM((64 * 24, LANES), F32),
            dma, dma((4,)), dma, dma((ep,)), dma, dma((ep,)), dma, dma, dma, dma((ep,)),
        ],
        compiler_params=pltpu.CompilerParams(collective_id=1, has_side_effects=True),
        name="mix",
    )(mixed, xraw, r, gain, wo, wg, wu, wd)


def rms_norm(values, gain):
    floats = values.astype(jnp.float32)
    return floats * lax.rsqrt(jnp.mean(floats * floats, axis=-1, keepdims=True) + 1e-06) * gain


def conv_step(window_state, newest, taps):
    window = jnp.concatenate([window_state, newest[:, None, :]], axis=1)
    mixed = jax.nn.silu(jnp.sum(window.astype(jnp.float32) * taps[None, :, :], axis=1))
    return (mixed, window[:, 1:])


def body(
    ep, tokens_in, mix_gain, w_gate_z, w_value, w_in_bc, w_step, step_bias, decay_log, skip_gain, conv_x_weight,
    conv_bc_weight, conv_x_state, conv_bc_state, ssm_state, inner_gain, out_weight, ffn_gain, expert_gate,
    expert_up, expert_down, routes, route_weight,
):
    seqs, width = tokens_in.shape
    r, xraw, st = project(
        ep, tokens_in.reshape(2, 32, LANES), mix_gain.reshape(32, LANES), w_gate_z, w_value, w_in_bc, w_step,
        routes, route_weight,
    )
    tiles = r.reshape(ep, 2, 4, LANES)
    z_pre = tiles[:, :, 0].transpose(1, 0, 2).reshape(seqs, -1)
    x_pre = tiles[:, :, 1].transpose(1, 0, 2).reshape(seqs, -1)
    bc_pre = tiles[:, :, 2].astype(F32).reshape(8, 4, 2, LANES).sum(1).astype(BF16)
    bc_pre = bc_pre.transpose(1, 0, 2).reshape(seqs, -1)
    me = lax.axis_index("ep")
    step_pre = lax.dynamic_slice_in_dim(st, me * 2, 2, 0)
    x_conv, new_conv_x = conv_step(conv_x_state, x_pre, conv_x_weight)
    bc_conv, new_conv_bc = conv_step(conv_bc_state, bc_pre, conv_bc_weight)
    group_cols = GROUPS * NSTATE
    in_map = jnp.repeat(bc_conv[:, :group_cols].reshape(seqs, GROUPS, NSTATE), HEADS // GROUPS, axis=1)
    out_map = jnp.repeat(bc_conv[:, group_cols:].reshape(seqs, GROUPS, NSTATE), HEADS // GROUPS, axis=1)
    step = jax.nn.softplus(step_pre + step_bias[None, :])
    decay = jnp.exp(-step * jnp.exp(decay_log)[None, :])
    x_heads = x_conv.reshape(seqs, HEADS, HEAD_DIM)
    new_state = (
        decay[:, :, None, None] * ssm_state + (step[:, :, None] * x_heads)[..., None] * in_map[:, :, None, :]
    )
    head_out = jnp.einsum("bhn,bhpn->bhp", out_map, new_state)
    head_out = head_out + skip_gain[None, :, None] * x_heads
    gated = head_out.reshape(seqs, HEADS * HEAD_DIM) * jax.nn.silu(z_pre.astype(jnp.float32))
    mixed = rms_norm(gated, inner_gain).astype(BF16)
    out = mix(
        ep, mixed.reshape(2, 32, LANES), xraw, r, ffn_gain.reshape(32, LANES), out_weight, expert_gate, expert_up,
        expert_down,
    )
    return out.reshape(seqs, width), new_state, new_conv_x, new_conv_bc


def solution(mesh):
    ep = mesh.shape["ep"]
    cols, rep = P(None, "ep"), P()
    placed = (
        P(GRP_EP, None), rep, cols, cols, cols, rep, rep, rep, rep, rep, rep,
        P(GRP_EP, None, None), P(GRP_EP, None, None), P(GRP_EP, None, None, None),
        rep, cols, rep, P("ep", None, None), P("ep", None, None), P("ep", None, None),
        P(GRP_EP, None), P(GRP_EP, None),
    )
    return jax.shard_map(
        functools.partial(body, ep),
        mesh=mesh,
        in_specs=placed,
        out_specs=(
            P(GRP_EP, None),
            P(GRP_EP, None, None, None),
            P(GRP_EP, None, None),
            P(GRP_EP, None, None),
        ),
        check_vma=False,
    )
```

```python
import functools

import jax
import jax.numpy as jnp
from jax import lax
from jax.experimental import pallas as pl
from jax.experimental.pallas import tpu as pltpu
from jax.sharding import PartitionSpec as P

TOPK = 4
GRP_EP = ("grp", "ep")
MESH = pl.DeviceIdType.MESH
F32 = jnp.float32
BF16 = jnp.bfloat16
LANES = 128
PITCH = 40

OWN = (6, -6, 3, -3, 1, -1)
RELAYS = (3, -3, 6, -6)


class Comm:
    def __init__(self, ep):
        self.ep = ep
        self.nz = ep // 2
        self.me = lax.axis_index("ep")
        self.core = lax.rem(self.me, 2)
        self.z = lax.div(self.me, 2)

    def at(self, offset, core):
        return lax.rem(self.z + offset + self.nz, self.nz) * 2 + core

    def partner(self):
        return self.z * 2 + (1 - self.core)

    def barrier(self):
        sem = pltpu.get_barrier_semaphore()

        def greet(i, carry):
            pl.semaphore_signal(
                sem, inc=1, device_id={"ep": lax.rem(self.me + i, self.ep)}, device_id_type=MESH
            )
            return carry

        lax.fori_loop(1, self.ep, greet, 0)
        return lambda: pl.semaphore_wait(sem, self.ep - 1)

    def copy(self, src, dst, send, recv, to):
        return pltpu.make_async_remote_copy(
            src_ref=src, dst_ref=dst, send_sem=send, recv_sem=recv, device_id={"ep": to}, device_id_type=MESH
        )

    def gather(self, buf, send, recv, landed):
        core, me = self.core, self.me

        def pass_on(block, to):
            self.copy(buf.at[block], buf.at[block], send, recv.at[block], to).start()

        def arrive(block):
            self.copy(buf.at[block], buf.at[block], send, recv.at[block], me).wait_recv()

        for d in OWN:
            pass_on(me, self.at(d, core))
        pass_on(me, self.partner())
        landed(me)
        extra = 2 - 4 * core
        for d in RELAYS:
            block = self.at(-d, core)
            arrive(block)
            pass_on(block, self.at(1, core))
            pass_on(block, self.at(-1, core))
            if d == 6:

                @pl.when(core == 0)
                def _(block=block):
                    pass_on(block, self.at(2, core))

            if d == -6:

                @pl.when(core == 1)
                def _(block=block):
                    pass_on(block, self.at(-2, core))

            pass_on(block, self.partner())
            landed(block)
        del extra
        for d in (1, -1, 2, -2, 4, -4, 5, -5, 7, -7, 8):
            block = self.at(-d, core)
            arrive(block)
            pass_on(block, self.partner())
            landed(block)

        def other(i, carry):
            block = self.at(i, 1 - core)
            arrive(block)
            landed(block)
            return carry

        lax.fori_loop(0, self.nz, other, 0)
        n = self.nz - 1 + self.nz
        whole = buf.at[pl.ds(0, n)]
        self.copy(whole, whole, send, recv.at[0], me).wait_send()

    def exchange(self, out, back, send, recv):
        me, ep, nz = self.me, self.ep, self.nz

        def one(to):
            self.copy(out.at[to], back.at[me], send, recv.at[me], to).start()

        def far_first(k, carry):
            offset = (nz // 2 - lax.div(k + 1, 2)) * (1 - 2 * lax.rem(k, 2))
            one(self.at(offset, 0))
            one(self.at(offset, 1))
            return carry

        lax.fori_loop(0, nz - 1, far_first, 0)
        one(self.partner())
        back[me] = out[me]

    def exchanged(self, out, back, send, recv, landed):
        me, ep = self.me, self.ep
        landed(me)

        def one(i, carry):
            frm = lax.rem(me + i, ep)
            self.copy(back.at[frm], back.at[frm], send, recv.at[frm], me).wait_recv()
            landed(frm)
            return carry

        lax.fori_loop(1, ep, one, 0)
        whole = out.at[pl.ds(0, ep - 1)]
        self.copy(whole, whole, send, recv.at[0], me).wait_send()


def tall(x, n):
    return x.reshape(n, x.shape[0] // n, x.shape[1])


def vmem():
    return pl.BlockSpec(memory_space=pltpu.VMEM)


def hbm():
    return pl.BlockSpec(memory_space=pl.ANY)


def smem():
    return pl.BlockSpec(memory_space=pltpu.SMEM)


def rows_of(dst, src, base):
    for j in range(src.shape[1] // LANES):
        dst[base + j : base + j + 1, :] = src[:, j * LANES : (j + 1) * LANES]


def row_of(dst, r, src, base, n):
    for j in range(n):
        dst[r : r + 1, j * LANES : (j + 1) * LANES] = src[base + j : base + j + 1, :]


def layer_kernel(
    ep, tok, mix_gain, wz_hbm, wx_hbm, wbc_hbm, wst_hbm, step_bias, decay_log, skip_gain, conv_x_w, conv_bc_w,
    conv_x, conv_bc, state_hbm, inner_gain, wo_hbm, ffn_gain, wg_hbm, wu_hbm, wd_hbm, routes, weights,
    out_ref, state_out, new_x, new_bc,
    buf, buf2, buf3, stage, lhs, xraw, wz, wx, wst, wo, wg, wu, wd, state, flat, out, back, tokf, convx, convbc,
    stepbc, decaybc, skipbc, bcs, ybuf, xbuf, rowx, rowbc, sq, act, wide, half_out, half_in, mine, total,
    send_rows, got_rows,
    wload, ssem, send1, recv1, send2, recv2, send3, recv3, hsend, hrecv, xsend, xrecv, csend, crecv,
):
    comm = Comm(ep)
    me, core = comm.me, comm.core
    ready = comm.barrier()
    pairs = (
        (wz_hbm, wz), (wx_hbm, wx), (wst_hbm, wst.at[pl.ds(0, 64)]), (wbc_hbm, wst.at[pl.ds(64, 32)]),
        (state_hbm, state), (wo_hbm, wo), (wg_hbm.at[0], wg), (wu_hbm.at[0], wu), (wd_hbm.at[0], wd),
    )
    pulls = [pltpu.make_async_copy(a, b, wload.at[i]) for i, (a, b) in enumerate(pairs)]
    for p in pulls:
        p.start()

    rows = tok[...].astype(F32)
    for r in range(2):
        rows_of(tokf, rows[r : r + 1, :], r * 32)
    buf[me] = tall(tokf[...], 2).astype(BF16)
    for conv, taps, dst, n in ((conv_x, conv_x_w, convx, 32), (conv_bc, conv_bc_w, convbc, 8)):
        old = conv[0].astype(F32) * taps[0:1, :]
        for c in range(1, 3):
            old = old + conv[c].astype(F32) * taps[c : c + 1, :]
        for r in range(2):
            rows_of(dst, old[r : r + 1, :], r * n)
        rows_of(dst, taps[3:4, :], 2 * n)
    lane = lax.broadcasted_iota(jnp.int32, (1, LANES), 1)
    dense = jnp.zeros((1, LANES), F32)
    for r in range(2):
        for k in range(TOPK):
            dense = dense + jnp.where(lane == routes[r, k] + 32 * r, weights[r, k], 0.0)
    high = dense.astype(BF16).astype(F32)
    flat[pl.ds(3, 32, stride=8), :] = jnp.broadcast_to(high, (32, LANES))
    flat[pl.ds(7, 32, stride=8), :] = jnp.broadcast_to(dense - high, (32, LANES))
    blank = jnp.zeros((1, 64), F32)

    def column(row):
        return jnp.transpose(jnp.broadcast_to(row, (LANES, LANES)))

    skipbc[...] = column(jnp.concatenate([skip_gain[...], blank], axis=1))
    sq[...] = jnp.zeros((64, LANES), F32)
    ready()

    def landed(block):
        both = buf[block].astype(F32)
        for r in range(2):
            stage[pl.ds(pl.multiple_of((block * 2 + r) * PITCH, 8), 32), :] = both[r]

    comm.gather(buf, send1, recv1, landed)
    square = jnp.zeros((64, LANES), F32)
    for j in range(32):
        x = stage[pl.ds(j, 64, stride=PITCH), :]
        square = square + x * x
        xraw[:, j * LANES : (j + 1) * LANES] = x.astype(BF16)
        lhs[:, j * LANES : (j + 1) * LANES] = (x * mix_gain[j : j + 1, :]).astype(BF16)
    scale = lax.rsqrt(jnp.sum(square, axis=1, keepdims=True) / 4096.0 + 1e-6)
    for p in pulls[:4]:
        p.wait()
    left = lhs[...]
    z = jnp.dot(left, wz[...], preferred_element_type=F32) * scale
    flat[pl.ds(0, 64, stride=4), :] = z
    x = jnp.dot(left, wx[...], preferred_element_type=F32) * scale
    flat[pl.ds(1, 64, stride=4), :] = x
    st = lax.dot_general(left, wst[...], (((1,), (1,)), ((), ())), preferred_element_type=F32) * scale
    bc = st[:, 64:96]
    spread = jnp.concatenate([bc, bc, bc, bc], axis=1)
    flat[pl.ds(2, 64, stride=4), :] = jnp.where(lax.div(lane, 32) == lax.rem(me, 4), spread, 0.0)
    out[...] = tall(flat[...], 32).astype(BF16)
    comm.exchange(out, back, xsend, xrecv)

    flat[pl.ds(0, 64, stride=4), :] = jnp.concatenate([st[:, 0:64], st[:, 0:64]], axis=1)
    mine8 = flat[pl.ds(pl.multiple_of(me * 8, 8), 8), :]
    bias = jnp.concatenate([step_bias[...], blank], axis=1)
    rate = jnp.exp(jnp.concatenate([decay_log[...], blank], axis=1))
    for r in range(2):
        step = jax.nn.softplus(mine8[r * 4 : r * 4 + 1, :] + bias)
        stepbc[pl.ds(r * LANES, LANES), :] = column(step)
        decaybc[pl.ds(r * LANES, LANES), :] = column(jnp.exp(-step * rate))
    comm.exchanged(out, back, xsend, xrecv, lambda frm: None)
    flat[...] = back[...].astype(F32).reshape(256, LANES)
    pulls[4].wait()

    low = lax.broadcasted_iota(jnp.int32, (32, LANES), 1) < 64
    for r in range(2):
        x_pre = flat[pl.ds(4 * r + 1, 32, stride=8), :]
        bc_pre = flat[pl.ds(4 * r + 2, 8, stride=32), :]
        for q in range(1, 4):
            bc_pre = bc_pre + flat[pl.ds(8 * q + 4 * r + 2, 8, stride=32), :]
        xbuf[pl.ds(r * 32, 32), :] = x_pre
        bcs[pl.ds(16 + r * 8, 8), :] = bc_pre
        xc = jax.nn.silu(convx[pl.ds(r * 32, 32), :] + convx[pl.ds(64, 32), :] * x_pre)
        bcs[pl.ds(r * 8, 8), :] = jax.nn.silu(convbc[pl.ds(r * 8, 8), :] + convbc[pl.ds(16, 8), :] * bc_pre)
        per = jnp.where(
            low,
            stepbc[pl.ds(r * LANES, 32, stride=2), :],
            stepbc[pl.ds(r * LANES + 1, 32, stride=2), :],
        )
        skip = jnp.where(low, skipbc[pl.ds(0, 32, stride=2), :], skipbc[pl.ds(1, 32, stride=2), :])
        total[pl.ds(r * 32, 32), :] = per * xc
        total[pl.ds(64 + r * 32, 32), :] = skip * xc

    def group(i, carry):
        r, g = lax.div(i, 4), lax.rem(i, 4)
        cols = jnp.transpose(total[pl.ds(pl.multiple_of(i * 8, 8), 8), :])
        into = jnp.broadcast_to(bcs[pl.ds(r * 8 + g, 1), :], (LANES, LANES))
        outof = jnp.broadcast_to(bcs[pl.ds(r * 8 + 4 + g, 1), :], (8, LANES)).astype(BF16)
        for k in range(8):
            h = g * 16 + 2 * k
            dec = jnp.concatenate(
                [
                    jnp.broadcast_to(decaybc[pl.ds(r * LANES + h, 1), :], (64, LANES)),
                    jnp.broadcast_to(decaybc[pl.ds(r * LANES + h + 1, 1), :], (64, LANES)),
                ],
                axis=0,
            )
            new = dec * state[r, pl.ds(h, 2)].reshape(LANES, LANES)
            new = new + jnp.broadcast_to(cols[:, k : k + 1], (LANES, LANES)) * into
            state[r, pl.ds(h, 2)] = new.reshape(2, 64, LANES)
            y = lax.dot_general(
                outof, new.astype(BF16), (((1,), (1,)), ((), ())), preferred_element_type=F32
            )
            ybuf[pl.ds(i * 8 + k, 1), :] = y[0:1, :]
        return carry

    lax.fori_loop(0, 8, group, 0)
    store = pltpu.make_async_copy(state, state_out, ssem)
    store.start()
    for r in range(2):
        at = pl.ds(r * 32, 32)
        gated = ybuf[at, :] + total[pl.ds(64 + r * 32, 32), :]
        gated = gated * jax.nn.silu(flat[pl.ds(4 * r, 32, stride=8), :])
        mean = jnp.sum(jnp.sum(gated * gated, axis=1, keepdims=True), axis=0, keepdims=True) / 4096.0
        buf2[me, r] = (gated * lax.rsqrt(mean + 1e-6) * inner_gain[...]).astype(BF16)

    def landed2(block):
        both = buf2[block].astype(F32)
        for r in range(2):
            stage[pl.ds(pl.multiple_of((block * 2 + r) * PITCH, 8), 32), :] = both[r]

    comm.gather(buf2, send2, recv2, landed2)
    for j in range(32):
        lhs[:, j * LANES : (j + 1) * LANES] = stage[pl.ds(j, 64, stride=PITCH), :].astype(BF16)
    pulls[5].wait()
    buf3[me] = jnp.dot(lhs[...], wo[...], preferred_element_type=F32).astype(BF16)

    def landed3(block):
        cols = pl.ds(pl.multiple_of(block * LANES, LANES), LANES)
        resid = (xraw[:, cols].astype(F32) + buf3[block].astype(F32)).astype(BF16).astype(F32)
        sq[...] = sq[...] + resid * resid
        stage[pl.ds(block, 64, stride=PITCH), :] = resid
        lhs[:, cols] = (resid * ffn_gain[pl.ds(block, 1), :]).astype(BF16)

    comm.gather(buf3, send3, recv3, landed3)
    scale = lax.rsqrt(jnp.sum(sq[...], axis=1, keepdims=True) / 4096.0 + 1e-6)
    pulls[6].wait()
    pulls[7].wait()
    left = lhs[...]
    gate = jnp.dot(left, wg[...], preferred_element_type=F32) * scale
    up = jnp.dot(left, wu[...], preferred_element_type=F32) * scale
    act[...] = (jax.nn.silu(gate) * up).astype(BF16)
    pulls[8].wait()
    lanes32 = lax.broadcasted_iota(jnp.int32, (32, LANES), 1)
    dense = flat[pl.ds(3, 32, stride=8), :] + flat[pl.ds(7, 32, stride=8), :]
    for r in range(2):
        picked = jnp.sum(jnp.where(lanes32 == me + 32 * r, dense, 0.0), axis=1, keepdims=True)
        wide[pl.ds(r, 32, stride=2), :] = jnp.broadcast_to(picked, (32, LANES))
    weight = jnp.concatenate([wide[...]] * 4, axis=1)

    def expert(half, k):
        cols = pl.ds(pl.multiple_of(half * 2048 + k * 512, 512), 512)
        y = jnp.dot(act[...], wd[:, cols], preferred_element_type=F32).astype(BF16).astype(F32)
        return y * weight

    for k in range(4):
        half_out[:, k * 512 : (k + 1) * 512] = expert(1 - core, k).astype(BF16)
    swap = comm.copy(half_out, half_in, hsend, hrecv, comm.partner())
    swap.start()
    for k in range(4):
        mine[:, k * 512 : (k + 1) * 512] = expert(core, k)
    swap.wait()
    for j in range(16):
        cols = slice(j * LANES, (j + 1) * LANES)
        total[pl.ds(j, 64, stride=24), :] = mine[:, cols] + half_in[:, cols].astype(F32)

    def pack(t, carry):
        for r in range(2):
            send_rows[t, r] = total[pl.ds(pl.multiple_of((t * 2 + r) * 24, 8), 16), :].astype(BF16)
        return carry

    lax.fori_loop(0, ep, pack, 0)
    comm.exchange(send_rows, got_rows, csend, crecv)
    for r in range(2):
        tokf[pl.ds(r * 32, 32), :] = stage[pl.ds(pl.multiple_of((me * 2 + r) * PITCH, 8), 32), :]
    for r in range(2):
        row_of(rowx, r, xbuf, r * 32, 32)
        row_of(rowbc, r, bcs, 16 + r * 8, 8)
    for old, new, row in ((conv_x, new_x, rowx), (conv_bc, new_bc, rowbc)):
        new[0] = old[1]
        new[1] = old[2]
        new[2] = row[...].astype(BF16)

    def arrived(frm):
        h = lax.rem(frm, 2)
        for r in range(2):
            at = pl.ds(pl.multiple_of(r * 32 + h * 16, 8), 16)
            tokf[at, :] = tokf[at, :] + got_rows[frm, r].astype(F32)

    comm.exchanged(send_rows, got_rows, csend, crecv, arrived)
    for r in range(2):
        row_of(rowx, r, tokf, r * 32, 32)
    out_ref[...] = rowx[...].astype(BF16)
    store.wait()


def layer(ep, *args):
    dma = pltpu.SemaphoreType.DMA
    v = pltpu.VMEM
    state = args[13]
    return pl.pallas_call(
        functools.partial(layer_kernel, ep),
        out_shape=(
            jax.ShapeDtypeStruct((2, 4096), BF16),
            jax.ShapeDtypeStruct(state.shape, F32),
            jax.ShapeDtypeStruct(args[11].shape, BF16),
            jax.ShapeDtypeStruct(args[12].shape, BF16),
        ),
        in_specs=[
            vmem(), vmem(), hbm(), hbm(), hbm(), hbm(), vmem(), vmem(), vmem(), vmem(), vmem(),
            vmem(), vmem(), hbm(), vmem(), hbm(), vmem(), hbm(), hbm(), hbm(), smem(), smem(),
        ],
        out_specs=(vmem(), hbm(), vmem(), vmem()),
        scratch_shapes=[
            v((ep, 2, 32, LANES), BF16), v((ep, 2, 32, LANES), BF16), v((ep, 64, LANES), BF16),
            v((64 * PITCH, LANES), F32), v((64, 4096), BF16), v((64, 4096), BF16),
            v((4096, LANES), BF16), v((4096, LANES), BF16), v((96, 4096), BF16), v((4096, LANES), BF16),
            v((4096, 512), BF16), v((4096, 512), BF16), v((512, 4096), BF16), v(state.shape, F32),
            v((256, LANES), F32), v((ep, 8, LANES), BF16), v((ep, 8, LANES), BF16), v((64, LANES), F32),
            v((96, LANES), F32), v((24, LANES), F32),
            v((256, LANES), F32), v((256, LANES), F32), v((LANES, LANES), F32), v((32, LANES), F32),
            v((64, LANES), F32), v((64, LANES), F32), v((2, 4096), F32), v((2, 1024), F32), v((64, LANES), F32),
            v((64, 512), BF16), v((64, LANES), F32), v((64, 2048), BF16), v((64, 2048), BF16),
            v((64, 2048), F32), v((64 * 24, LANES), F32),
            v((ep, 2, 16, LANES), BF16), v((ep, 2, 16, LANES), BF16),
            dma((9,)), dma, dma, dma((ep,)), dma, dma((ep,)), dma, dma((ep,)), dma, dma, dma, dma((ep,)),
            dma, dma((ep,)),
        ],
        compiler_params=pltpu.CompilerParams(collective_id=0, has_side_effects=True),
        name="layer",
    )(*args)


def body(
    ep, tokens_in, mix_gain, w_gate_z, w_value, w_in_bc, w_step, step_bias, decay_log, skip_gain, conv_x_weight,
    conv_bc_weight, conv_x_state, conv_bc_state, ssm_state, inner_gain, out_weight, ffn_gain, expert_gate,
    expert_up, expert_down, routes, route_weight,
):
    out, new_state, new_x, new_bc = layer(
        ep, tokens_in, mix_gain.reshape(32, LANES), w_gate_z, w_value, w_in_bc.T, w_step.T,
        step_bias.reshape(1, 64), decay_log.reshape(1, 64), skip_gain.reshape(1, 64), conv_x_weight,
        conv_bc_weight, conv_x_state.transpose(1, 0, 2), conv_bc_state.transpose(1, 0, 2), ssm_state,
        inner_gain.reshape(32, LANES), out_weight, ffn_gain.reshape(32, LANES), expert_gate, expert_up,
        expert_down, routes, route_weight,
    )
    return out, new_state, new_x.transpose(1, 0, 2), new_bc.transpose(1, 0, 2)


def solution(mesh):
    ep = mesh.shape["ep"]
    cols, rep = P(None, "ep"), P()
    placed = (
        P(GRP_EP, None), rep, cols, cols, cols, rep, rep, rep, rep, rep, rep,
        P(GRP_EP, None, None), P(GRP_EP, None, None), P(GRP_EP, None, None, None),
        rep, cols, rep, P("ep", None, None), P("ep", None, None), P("ep", None, None),
        P(GRP_EP, None), P(GRP_EP, None),
    )
    return jax.shard_map(
        functools.partial(body, ep),
        mesh=mesh,
        in_specs=placed,
        out_specs=(
            P(GRP_EP, None),
            P(GRP_EP, None, None, None),
            P(GRP_EP, None, None),
            P(GRP_EP, None, None),
        ),
        check_vma=False,
    )
```

```python
import functools

import jax
import jax.numpy as jnp
from jax import lax
from jax.experimental import pallas as pl
from jax.experimental.pallas import tpu as pltpu
from jax.sharding import PartitionSpec as P

TOPK = 4
GRP_EP = ("grp", "ep")
MESH = pl.DeviceIdType.MESH
F32 = jnp.float32
BF16 = jnp.bfloat16
LANES = 128
PITCH = 40
VMEM_LIMIT = 34 * 1024 * 1024

OWN = (6, -6, 3, -3, 1, -1)
RELAYS = ((3, (1, -1)), (-3, (1, -1)), (6, (2, 1, -1)), (-6, (1, -1)))
LEAVES = (1, -1, 2, -2, 4, -4, 5, -5, 7, -7, 8)


class Comm:
    def __init__(self, ep):
        self.ep = ep
        self.nz = ep // 2
        self.me = lax.axis_index("ep")
        self.core = lax.rem(self.me, 2)
        self.z = lax.div(self.me, 2)

    def at(self, offset, core):
        return lax.rem(self.z + offset + self.nz, self.nz) * 2 + core

    def partner(self):
        return self.z * 2 + (1 - self.core)

    def barrier(self):
        sem = pltpu.get_barrier_semaphore()

        def greet(i, carry):
            pl.semaphore_signal(
                sem, inc=1, device_id={"ep": lax.rem(self.me + i, self.ep)}, device_id_type=MESH
            )
            return carry

        lax.fori_loop(1, self.ep, greet, 0)
        return lambda: pl.semaphore_wait(sem, self.ep - 1)

    def copy(self, src, dst, send, recv, to):
        return pltpu.make_async_remote_copy(
            src_ref=src, dst_ref=dst, send_sem=send, recv_sem=recv, device_id={"ep": to}, device_id_type=MESH
        )

    def gather(self, buf, send, recv, landed):
        core, me = self.core, self.me

        def pass_on(block, to):
            self.copy(buf.at[block], buf.at[block], send, recv.at[block], to).start()

        def arrive(block):
            self.copy(buf.at[block], buf.at[block], send, recv.at[block], me).wait_recv()

        def sent(n):
            whole = buf.at[pl.ds(0, n)]
            self.copy(whole, whole, send, recv.at[0], me).wait_send()

        def turned(d, side):
            return d if side == 0 else -d

        for d in OWN:
            pass_on(me, self.at(d * (1 - 2 * core), 1))
        pass_on(me, self.partner())
        landed(me)
        steps = RELAYS + tuple((d, ()) for d in LEAVES)

        @pl.when(core == 1)
        def _():
            passed = 0
            for d, onward in steps:
                for side in range(2):
                    block = self.at(-turned(d, side), side)
                    arrive(block)
                    for step in onward:
                        pass_on(block, self.at(turned(step, side), 1))
                    pass_on(block, self.partner())
                    passed += len(onward) + 1
                    landed(block)
            arrive(self.partner())
            landed(self.partner())
            sent(len(OWN) + 1)
            for start in range(0, passed, self.ep):
                sent(min(self.ep, passed - start))

        @pl.when(core == 0)
        def _():
            arrive(self.partner())
            landed(self.partner())
            for d, _ in steps:
                for side in range(2):
                    block = self.at(-turned(d, side), side)
                    arrive(block)
                    landed(block)
            sent(len(OWN) + 1)

    def exchange(self, out, back, send, recv):
        me, ep, nz = self.me, self.ep, self.nz

        def one(to):
            self.copy(out.at[to], back.at[me], send, recv.at[me], to).start()

        def far_first(k, carry):
            offset = (nz // 2 - lax.div(k + 1, 2)) * (1 - 2 * lax.rem(k, 2))
            one(self.at(offset, 0))
            one(self.at(offset, 1))
            return carry

        lax.fori_loop(0, nz - 1, far_first, 0)
        one(self.partner())
        back[me] = out[me]

    def exchanged(self, out, back, send, recv, landed):
        me, ep = self.me, self.ep
        landed(me)

        def one(i, carry):
            frm = lax.rem(me + i, ep)
            self.copy(back.at[frm], back.at[frm], send, recv.at[frm], me).wait_recv()
            landed(frm)
            return carry

        lax.fori_loop(1, ep, one, 0)
        whole = out.at[pl.ds(0, ep - 1)]
        self.copy(whole, whole, send, recv.at[0], me).wait_send()


def tall(x, n):
    return x.reshape(n, x.shape[0] // n, x.shape[1])


def vmem():
    return pl.BlockSpec(memory_space=pltpu.VMEM)


def hbm():
    return pl.BlockSpec(memory_space=pl.ANY)


def smem():
    return pl.BlockSpec(memory_space=pltpu.SMEM)


def rows_of(dst, src, base):
    for j in range(src.shape[1] // LANES):
        dst[base + j : base + j + 1, :] = src[:, j * LANES : (j + 1) * LANES]


def row_of(dst, r, src, base, n):
    for j in range(n):
        dst[r : r + 1, j * LANES : (j + 1) * LANES] = src[base + j : base + j + 1, :]


def layer_kernel(ep, n_in, n_out, *refs):
    inputs, outputs, locals_, refs = (
        refs[:n_in], refs[n_in : n_in + n_out], refs[n_in + n_out : 2 * n_in + n_out - 1], refs[2 * n_in + n_out - 1 :]
    )
    (
        tok, mix_gain, wz, wx, wst, step_bias, decay_log, skip_gain, conv_x_w, conv_bc_w, conv_x, conv_bc, _,
        inner_gain, wo, ffn_gain, wg, wu, wd, routes, weights,
    ) = locals_
    out_ref, state, new_x, new_bc = outputs
    (
        buf, buf2, buf3, stage, lhs, xraw, flat, out, back, tokf, convx, convbc,
        stepbc, decaybc, skipbc, bcs, ybuf, xbuf, rowx, rowbc, sq, act, wide, half_out, half_in, mine, total,
        send_rows, got_rows,
        wload, send1, recv1, send2, recv2, send3, recv3, hsend, hrecv, xsend, xrecv, csend, crecv,
    ) = refs
    comm = Comm(ep)
    me, core = comm.me, comm.core
    ready = comm.barrier()
    (
        tok_h, mix_h, wz_h, wx_h, wbc_h, wst_h, bias_h, decay_h, skip_h, cxw_h, cbw_h, cx_h, cb_h, state_h, inner_h,
        wo_h, ffn_h, wg_h, wu_h, wd_h, routes_h, weights_h,
    ) = inputs
    pairs = (
        (tok_h, tok), (cx_h, conv_x), (cxw_h, conv_x_w), (cb_h, conv_bc), (cbw_h, conv_bc_w), (routes_h, routes),
        (weights_h, weights), (skip_h, skip_gain), (bias_h, step_bias), (decay_h, decay_log), (mix_h, mix_gain),
        (inner_h, inner_gain), (ffn_h, ffn_gain),
        (wz_h, wz), (wx_h, wx), (wst_h, wst.at[pl.ds(0, 64)]), (wbc_h, wst.at[pl.ds(64, 32)]),
        (state_h, state), (wo_h, wo), (wg_h.at[0], wg), (wu_h.at[0], wu), (wd_h.at[0], wd),
    )
    pulls = [pltpu.make_async_copy(a, b, wload.at[i]) for i, (a, b) in enumerate(pairs)]
    for p in pulls:
        p.start()
    early, pulls = pulls[:13], pulls[13:]
    early[0].wait()

    rows = tok[...].astype(F32)
    for r in range(2):
        rows_of(tokf, rows[r : r + 1, :], r * 32)
    buf[me] = tall(tokf[...], 2).astype(BF16)
    for p in early[1:]:
        p.wait()
    for conv, taps, dst, n in ((conv_x, conv_x_w, convx, 32), (conv_bc, conv_bc_w, convbc, 8)):
        old = conv[0].astype(F32) * taps[0:1, :]
        for c in range(1, 3):
            old = old + conv[c].astype(F32) * taps[c : c + 1, :]
        for r in range(2):
            rows_of(dst, old[r : r + 1, :], r * n)
        rows_of(dst, taps[3:4, :], 2 * n)
    lane = lax.broadcasted_iota(jnp.int32, (1, LANES), 1)
    dense = jnp.zeros((1, LANES), F32)
    for r in range(2):
        for k in range(TOPK):
            dense = dense + jnp.where(lane == routes[r, k] + 32 * r, weights[r, k], 0.0)
    high = dense.astype(BF16).astype(F32)
    flat[pl.ds(3, 32, stride=8), :] = jnp.broadcast_to(high, (32, LANES))
    flat[pl.ds(7, 32, stride=8), :] = jnp.broadcast_to(dense - high, (32, LANES))
    blank = jnp.zeros((1, 64), F32)

    def column(row):
        return jnp.transpose(jnp.broadcast_to(row, (LANES, LANES)))

    skipbc[...] = column(jnp.concatenate([skip_gain[...], blank], axis=1))
    sq[...] = jnp.zeros((64, LANES), F32)
    ready()

    def landed(block):
        both = buf[block].astype(F32)
        for r in range(2):
            stage[pl.ds(pl.multiple_of((block * 2 + r) * PITCH, 8), 32), :] = both[r]

    comm.gather(buf, send1, recv1, landed)
    for p in pulls[:4]:
        p.wait()
    square = jnp.zeros((64, LANES), F32)
    z, x, st = jnp.zeros((64, LANES), F32), jnp.zeros((64, LANES), F32), jnp.zeros((64, 96), F32)
    for k in range(16):
        part = []
        for j in (2 * k, 2 * k + 1):
            chunk = stage[pl.ds(j, 64, stride=PITCH), :]
            square = square + chunk * chunk
            xraw[:, j * LANES : (j + 1) * LANES] = chunk.astype(BF16)
            part.append((chunk * mix_gain[j : j + 1, :]).astype(BF16))
        part = jnp.concatenate(part, axis=1)
        at = slice(k * 256, (k + 1) * 256)
        z = z + jnp.dot(part, wz[at, :], preferred_element_type=F32)
        x = x + jnp.dot(part, wx[at, :], preferred_element_type=F32)
        st = st + lax.dot_general(part, wst[:, at], (((1,), (1,)), ((), ())), preferred_element_type=F32)
    scale = lax.rsqrt(jnp.sum(square, axis=1, keepdims=True) / 4096.0 + 1e-6)
    z, x, st = z * scale, x * scale, st * scale
    flat[pl.ds(0, 64, stride=4), :] = z
    flat[pl.ds(1, 64, stride=4), :] = x
    bc = st[:, 64:96]
    spread = jnp.concatenate([bc, bc, bc, bc], axis=1)
    flat[pl.ds(2, 64, stride=4), :] = jnp.where(lax.div(lane, 32) == lax.rem(me, 4), spread, 0.0)
    out[...] = tall(flat[...], 32).astype(BF16)
    comm.exchange(out, back, xsend, xrecv)

    flat[pl.ds(0, 64, stride=4), :] = jnp.concatenate([st[:, 0:64], st[:, 0:64]], axis=1)
    mine8 = flat[pl.ds(pl.multiple_of(me * 8, 8), 8), :]
    bias = jnp.concatenate([step_bias[...], blank], axis=1)
    rate = jnp.exp(jnp.concatenate([decay_log[...], blank], axis=1))
    for r in range(2):
        step = jax.nn.softplus(mine8[r * 4 : r * 4 + 1, :] + bias)
        stepbc[pl.ds(r * LANES, LANES), :] = column(step)
        decaybc[pl.ds(r * LANES, LANES), :] = column(jnp.exp(-step * rate))
    comm.exchanged(out, back, xsend, xrecv, lambda frm: None)
    flat[...] = back[...].astype(F32).reshape(256, LANES)
    pulls[4].wait()

    low = lax.broadcasted_iota(jnp.int32, (32, LANES), 1) < 64
    for r in range(2):
        x_pre = flat[pl.ds(4 * r + 1, 32, stride=8), :]
        bc_pre = flat[pl.ds(4 * r + 2, 8, stride=32), :]
        for q in range(1, 4):
            bc_pre = bc_pre + flat[pl.ds(8 * q + 4 * r + 2, 8, stride=32), :]
        xbuf[pl.ds(r * 32, 32), :] = x_pre
        bcs[pl.ds(16 + r * 8, 8), :] = bc_pre
        xc = jax.nn.silu(convx[pl.ds(r * 32, 32), :] + convx[pl.ds(64, 32), :] * x_pre)
        bcs[pl.ds(r * 8, 8), :] = jax.nn.silu(convbc[pl.ds(r * 8, 8), :] + convbc[pl.ds(16, 8), :] * bc_pre)
        per = jnp.where(
            low,
            stepbc[pl.ds(r * LANES, 32, stride=2), :],
            stepbc[pl.ds(r * LANES + 1, 32, stride=2), :],
        )
        skip = jnp.where(low, skipbc[pl.ds(0, 32, stride=2), :], skipbc[pl.ds(1, 32, stride=2), :])
        total[pl.ds(r * 32, 32), :] = per * xc
        total[pl.ds(64 + r * 32, 32), :] = skip * xc

    def group(i, carry):
        r, g = lax.div(i, 4), lax.rem(i, 4)
        cols = jnp.transpose(total[pl.ds(pl.multiple_of(i * 8, 8), 8), :])
        into = jnp.broadcast_to(bcs[pl.ds(r * 8 + g, 1), :], (LANES, LANES))
        outof = jnp.broadcast_to(bcs[pl.ds(r * 8 + 4 + g, 1), :], (8, LANES)).astype(BF16)
        for k in range(8):
            h = g * 16 + 2 * k
            dec = jnp.concatenate(
                [
                    jnp.broadcast_to(decaybc[pl.ds(r * LANES + h, 1), :], (64, LANES)),
                    jnp.broadcast_to(decaybc[pl.ds(r * LANES + h + 1, 1), :], (64, LANES)),
                ],
                axis=0,
            )
            new = dec * state[r, pl.ds(h, 2)].reshape(LANES, LANES)
            new = new + jnp.broadcast_to(cols[:, k : k + 1], (LANES, LANES)) * into
            state[r, pl.ds(h, 2)] = new.reshape(2, 64, LANES)
            y = lax.dot_general(
                outof, new.astype(BF16), (((1,), (1,)), ((), ())), preferred_element_type=F32
            )
            ybuf[pl.ds(i * 8 + k, 1), :] = y[0:1, :]
        return carry

    lax.fori_loop(0, 8, group, 0)
    for r in range(2):
        at = pl.ds(r * 32, 32)
        gated = ybuf[at, :] + total[pl.ds(64 + r * 32, 32), :]
        gated = gated * jax.nn.silu(flat[pl.ds(4 * r, 32, stride=8), :])
        mean = jnp.sum(jnp.sum(gated * gated, axis=1, keepdims=True), axis=0, keepdims=True) / 4096.0
        buf2[me, r] = (gated * lax.rsqrt(mean + 1e-6) * inner_gain[...]).astype(BF16)

    def landed2(block):
        both = buf2[block].astype(F32)
        for r in range(2):
            stage[pl.ds(pl.multiple_of((block * 2 + r) * PITCH, 8), 32), :] = both[r]

    comm.gather(buf2, send2, recv2, landed2)
    pulls[5].wait()
    cols_out = jnp.zeros((64, LANES), F32)
    for k in range(16):
        part = [stage[pl.ds(j, 64, stride=PITCH), :].astype(BF16) for j in (2 * k, 2 * k + 1)]
        part = jnp.concatenate(part, axis=1)
        cols_out = cols_out + jnp.dot(part, wo[k * 256 : (k + 1) * 256, :], preferred_element_type=F32)
    buf3[me] = cols_out.astype(BF16)

    def landed3(block):
        cols = pl.ds(pl.multiple_of(block * LANES, LANES), LANES)
        resid = (xraw[:, cols].astype(F32) + buf3[block].astype(F32)).astype(BF16).astype(F32)
        sq[...] = sq[...] + resid * resid
        stage[pl.ds(block, 64, stride=PITCH), :] = resid
        lhs[:, cols] = (resid * ffn_gain[pl.ds(block, 1), :]).astype(BF16)

    comm.gather(buf3, send3, recv3, landed3)
    scale = lax.rsqrt(jnp.sum(sq[...], axis=1, keepdims=True) / 4096.0 + 1e-6)
    pulls[6].wait()
    pulls[7].wait()
    left = lhs[...]
    gate = jnp.dot(left, wg[...], preferred_element_type=F32) * scale
    up = jnp.dot(left, wu[...], preferred_element_type=F32) * scale
    act[...] = (jax.nn.silu(gate) * up).astype(BF16)
    pulls[8].wait()
    lanes32 = lax.broadcasted_iota(jnp.int32, (32, LANES), 1)
    dense = flat[pl.ds(3, 32, stride=8), :] + flat[pl.ds(7, 32, stride=8), :]
    for r in range(2):
        picked = jnp.sum(jnp.where(lanes32 == me + 32 * r, dense, 0.0), axis=1, keepdims=True)
        wide[pl.ds(r, 32, stride=2), :] = jnp.broadcast_to(picked, (32, LANES))
    weight = jnp.concatenate([wide[...]] * 4, axis=1)

    def expert(half, k):
        cols = pl.ds(pl.multiple_of(half * 2048 + k * 512, 512), 512)
        y = jnp.dot(act[...], wd[:, cols], preferred_element_type=F32).astype(BF16).astype(F32)
        return y * weight

    for k in range(4):
        half_out[:, k * 512 : (k + 1) * 512] = expert(1 - core, k).astype(BF16)
    swap = comm.copy(half_out, half_in, hsend, hrecv, comm.partner())
    swap.start()
    for k in range(4):
        mine[:, k * 512 : (k + 1) * 512] = expert(core, k)
    swap.wait()
    for j in range(16):
        cols = slice(j * LANES, (j + 1) * LANES)
        total[pl.ds(j, 64, stride=24), :] = mine[:, cols] + half_in[:, cols].astype(F32)

    def pack(t, carry):
        for r in range(2):
            send_rows[t, r] = total[pl.ds(pl.multiple_of((t * 2 + r) * 24, 8), 16), :].astype(BF16)
        return carry

    lax.fori_loop(0, ep, pack, 0)
    comm.exchange(send_rows, got_rows, csend, crecv)
    for r in range(2):
        tokf[pl.ds(r * 32, 32), :] = stage[pl.ds(pl.multiple_of((me * 2 + r) * PITCH, 8), 32), :]
    for r in range(2):
        row_of(rowx, r, xbuf, r * 32, 32)
        row_of(rowbc, r, bcs, 16 + r * 8, 8)
    for old, new, row in ((conv_x, new_x, rowx), (conv_bc, new_bc, rowbc)):
        new[0] = old[1]
        new[1] = old[2]
        new[2] = row[...].astype(BF16)

    def arrived(frm):
        h = lax.rem(frm, 2)
        for r in range(2):
            at = pl.ds(pl.multiple_of(r * 32 + h * 16, 8), 16)
            tokf[at, :] = tokf[at, :] + got_rows[frm, r].astype(F32)

    comm.exchanged(send_rows, got_rows, csend, crecv, arrived)
    for r in range(2):
        row_of(rowx, r, tokf, r * 32, 32)
    out_ref[...] = rowx[...].astype(BF16)


def layer(ep, *args):
    dma = pltpu.SemaphoreType.DMA
    v = pltpu.VMEM
    local = [v(a.shape[1:] if a.shape[0] == 1 and a.ndim == 3 else a.shape, a.dtype) for a in args]
    local[4:6] = [v((96, 4096), BF16)]
    del local[12]
    local.insert(12, v((8, LANES), F32))
    local[-2:] = [pltpu.SMEM(a.shape, a.dtype) for a in args[-2:]]
    outs = (
        jax.ShapeDtypeStruct((2, 4096), BF16),
        jax.ShapeDtypeStruct(args[13].shape, F32),
        jax.ShapeDtypeStruct(args[11].shape, BF16),
        jax.ShapeDtypeStruct(args[12].shape, BF16),
    )
    results = pl.pallas_call(
        functools.partial(layer_kernel, ep, len(args), len(outs)),
        out_shape=outs,
        in_specs=[hbm()] * len(args),
        out_specs=(vmem(),) * len(outs),
        scratch_shapes=[
            *local,
            v((ep, 2, 32, LANES), BF16), v((ep, 2, 32, LANES), BF16), v((ep, 64, LANES), BF16),
            v((64 * PITCH, LANES), F32), v((64, 4096), BF16), v((64, 4096), BF16),
            v((256, LANES), F32), v((ep, 8, LANES), BF16), v((ep, 8, LANES), BF16), v((64, LANES), F32),
            v((96, LANES), F32), v((24, LANES), F32),
            v((256, LANES), F32), v((256, LANES), F32), v((LANES, LANES), F32), v((32, LANES), F32),
            v((64, LANES), F32), v((64, LANES), F32), v((2, 4096), F32), v((2, 1024), F32), v((64, LANES), F32),
            v((64, 512), BF16), v((64, LANES), F32), v((64, 2048), BF16), v((64, 2048), BF16),
            v((64, 2048), F32), v((64 * 24, LANES), F32),
            v((ep, 2, 16, LANES), BF16), v((ep, 2, 16, LANES), BF16),
            dma((22,)), dma, dma((ep,)), dma, dma((ep,)), dma, dma((ep,)), dma, dma, dma, dma((ep,)),
            dma, dma((ep,)),
        ],
        compiler_params=pltpu.CompilerParams(
            collective_id=0, has_side_effects=True, vmem_limit_bytes=VMEM_LIMIT
        ),
        name="layer",
    )(*(pltpu.with_memory_space_constraint(a, pltpu.HBM) for a in args))
    return pl.pallas_call(
        flush_kernel,
        out_shape=outs,
        in_specs=[vmem()] * len(outs),
        out_specs=(hbm(),) * len(outs),
        scratch_shapes=[dma((len(outs),))],
        compiler_params=pltpu.CompilerParams(vmem_limit_bytes=1024 * 1024),
        name="flush",
    )(*results)


def flush_kernel(*refs):
    n = len(refs) // 2
    copies = [pltpu.make_async_copy(refs[i], refs[n + i], refs[-1].at[i]) for i in range(n)]
    for c in copies:
        c.start()
    for c in copies:
        c.wait()


def body(
    ep, tokens_in, mix_gain, w_gate_z, w_value, w_in_bc, w_step, step_bias, decay_log, skip_gain, conv_x_weight,
    conv_bc_weight, conv_x_state, conv_bc_state, ssm_state, inner_gain, out_weight, ffn_gain, expert_gate,
    expert_up, expert_down, routes, route_weight,
):
    out, new_state, new_x, new_bc = layer(
        ep, tokens_in, mix_gain.reshape(32, LANES), w_gate_z, w_value, w_in_bc.T, w_step.T,
        step_bias.reshape(1, 64), decay_log.reshape(1, 64), skip_gain.reshape(1, 64), conv_x_weight,
        conv_bc_weight, conv_x_state.transpose(1, 0, 2), conv_bc_state.transpose(1, 0, 2), ssm_state,
        inner_gain.reshape(32, LANES), out_weight, ffn_gain.reshape(32, LANES), expert_gate, expert_up,
        expert_down, routes, route_weight,
    )
    return out, new_state, new_x.transpose(1, 0, 2), new_bc.transpose(1, 0, 2)


def solution(mesh):
    ep = mesh.shape["ep"]
    cols, rep = P(None, "ep"), P()
    placed = (
        P(GRP_EP, None), rep, cols, cols, cols, rep, rep, rep, rep, rep, rep,
        P(GRP_EP, None, None), P(GRP_EP, None, None), P(GRP_EP, None, None, None),
        rep, cols, rep, P("ep", None, None), P("ep", None, None), P("ep", None, None),
        P(GRP_EP, None), P(GRP_EP, None),
    )
    return jax.shard_map(
        functools.partial(body, ep),
        mesh=mesh,
        in_specs=placed,
        out_specs=(
            P(GRP_EP, None),
            P(GRP_EP, None, None, None),
            P(GRP_EP, None, None),
            P(GRP_EP, None, None),
        ),
        check_vma=False,
    )
```

```python
import functools

import jax
import jax.numpy as jnp
from jax import lax
from jax.experimental import pallas as pl
from jax.experimental.pallas import tpu as pltpu
from jax.sharding import PartitionSpec as P

TOPK = 4
GRP_EP = ("grp", "ep")
MESH = pl.DeviceIdType.MESH
F32 = jnp.float32
BF16 = jnp.bfloat16
LANES = 128
PITCH = 40
VMEM_LIMIT = 38 * 1024 * 1024

OWN = (6, -6, 3, -3, 1, -1)
RELAYS = ((3, (1, -1)), (-3, (1, -1)), (6, (2, 1, -1)), (-6, (1, -1)))
GREET = (1, -1, 2, -2, 3, -3, 6, -6)
LEAVES = (1, -1, 2, -2, 4, -4, 5, -5, 7, -7, 8)


class Comm:
    def __init__(self, ep):
        self.ep = ep
        self.nz = ep // 2
        self.me = lax.axis_index("ep")
        self.core = lax.rem(self.me, 2)
        self.z = lax.div(self.me, 2)

    def at(self, offset, core):
        return lax.rem(self.z + offset + self.nz, self.nz) * 2 + core

    def partner(self):
        return self.z * 2 + (1 - self.core)

    def barrier(self):
        sem = pltpu.get_barrier_semaphore()

        def greet(to):
            pl.semaphore_signal(sem, inc=1, device_id={"ep": to}, device_id_type=MESH)

        @pl.when(self.core == 1)
        def _():
            for d in GREET:
                greet(self.at(d, 0))
                greet(self.at(d, 1))

        greet(self.partner())
        return lambda: pl.semaphore_wait(sem, len(GREET) + 1)

    def copy(self, src, dst, send, recv, to):
        return pltpu.make_async_remote_copy(
            src_ref=src, dst_ref=dst, send_sem=send, recv_sem=recv, device_id={"ep": to}, device_id_type=MESH
        )

    def gather_start(self, buf, send, recv):
        me = self.me
        for to in [self.at(d * (1 - 2 * self.core), 1) for d in OWN] + [self.partner()]:
            self.copy(buf.at[me], buf.at[me], send, recv.at[me], to).start()

    def gather(self, buf, send, recv, landed):
        core, me = self.core, self.me

        def pass_on(block, to):
            self.copy(buf.at[block], buf.at[block], send, recv.at[block], to).start()

        def arrive(block):
            self.copy(buf.at[block], buf.at[block], send, recv.at[block], me).wait_recv()

        def sent(n):
            whole = buf.at[pl.ds(0, n)]
            self.copy(whole, whole, send, recv.at[0], me).wait_send()

        def turned(d, side):
            return d if side == 0 else -d

        steps = RELAYS + tuple((d, ()) for d in LEAVES)
        arrive(self.partner())
        landed(me, self.partner())

        @pl.when(core == 1)
        def _():
            passed = 0
            for d, onward in steps:
                blocks = [self.at(-turned(d, side), side) for side in range(2)]
                for side, block in enumerate(blocks):
                    arrive(block)
                    for step in onward:
                        pass_on(block, self.at(turned(step, side), 1))
                    pass_on(block, self.partner())
                    passed += len(onward) + 1
                landed(*blocks)
            sent(len(OWN) + 1)
            for start in range(0, passed, self.ep):
                sent(min(self.ep, passed - start))

        @pl.when(core == 0)
        def _():
            for d, _ in steps:
                blocks = [self.at(-turned(d, side), side) for side in range(2)]
                for block in blocks:
                    arrive(block)
                landed(*blocks)
            sent(len(OWN) + 1)

    def exchange(self, out, back, send, recv):
        me, ep, nz = self.me, self.ep, self.nz

        def one(to):
            self.copy(out.at[to], back.at[me], send, recv.at[me], to).start()

        def far_first(k, carry):
            offset = (nz // 2 - lax.div(k + 1, 2)) * (1 - 2 * lax.rem(k, 2))
            one(self.at(offset, 0))
            one(self.at(offset, 1))
            return carry

        lax.fori_loop(0, nz - 1, far_first, 0)
        one(self.partner())
        back[me] = out[me]

    def exchanged(self, out, back, send, recv, landed):
        me, ep = self.me, self.ep
        landed(me)

        def one(i, carry):
            frm = lax.rem(me + i, ep)
            self.copy(back.at[frm], back.at[frm], send, recv.at[frm], me).wait_recv()
            landed(frm)
            return carry

        lax.fori_loop(1, ep, one, 0)
        whole = out.at[pl.ds(0, ep - 1)]
        self.copy(whole, whole, send, recv.at[0], me).wait_send()


def tall(x, n):
    return x.reshape(n, x.shape[0] // n, x.shape[1])


def vmem():
    return pl.BlockSpec(memory_space=pltpu.VMEM)


def hbm():
    return pl.BlockSpec(memory_space=pl.ANY)


def smem():
    return pl.BlockSpec(memory_space=pltpu.SMEM)


def rows_of(dst, src, base):
    for j in range(src.shape[1] // LANES):
        dst[base + j : base + j + 1, :] = src[:, j * LANES : (j + 1) * LANES]


def row_of(dst, r, src, base, n):
    for j in range(n):
        dst[r : r + 1, j * LANES : (j + 1) * LANES] = src[base + j : base + j + 1, :]


def layer_kernel(ep, n_in, n_out, *refs):
    inputs, outputs, locals_, refs = (
        refs[:n_in], refs[n_in : n_in + n_out], refs[n_in + n_out : 2 * n_in + n_out - 1], refs[2 * n_in + n_out - 1 :]
    )
    (
        tok, mix_gain, wz, wx, wst, step_bias, decay_log, skip_gain, conv_x_w, conv_bc_w, conv_x, conv_bc, _,
        inner_gain, wo, ffn_gain, wg, wu, wd, routes, weights,
    ) = locals_
    out_ref, state, new_x, new_bc = outputs
    (
        buf, buf2, buf3, stage, narrowed, gacc, xraw, flat, out, back, tokf, convx, convbc,
        stepbc, decaybc, skipbc, bcs, ybuf, xbuf, rowx, rowbc, sq, act, wide, half_out, half_in, total,
        send_rows, got_rows,
        wload, send1, recv1, send2, recv2, send3, recv3, hsend, hrecv, xsend, xrecv, csend, crecv,
    ) = refs
    comm = Comm(ep)
    me, core = comm.me, comm.core
    ready = comm.barrier()
    (
        tok_h, mix_h, wz_h, wx_h, wbc_h, wst_h, bias_h, decay_h, skip_h, cxw_h, cbw_h, cx_h, cb_h, state_h, inner_h,
        wo_h, ffn_h, wg_h, wu_h, wd_h, routes_h, weights_h,
    ) = inputs
    pairs = (
        (tok_h, tok), (cx_h, conv_x), (cxw_h, conv_x_w), (cb_h, conv_bc), (cbw_h, conv_bc_w), (routes_h, routes),
        (weights_h, weights), (skip_h, skip_gain), (bias_h, step_bias), (decay_h, decay_log), (mix_h, mix_gain),
        (inner_h, inner_gain), (ffn_h, ffn_gain),
        (wz_h, wz), (wx_h, wx), (wst_h, wst.at[pl.ds(0, 64)]), (wbc_h, wst.at[pl.ds(64, 32)]),
        (state_h, state), (wo_h, wo), (wg_h.at[0], wg), (wu_h.at[0], wu), (wd_h.at[0], wd),
    )
    pulls = [pltpu.make_async_copy(a, b, wload.at[i]) for i, (a, b) in enumerate(pairs)]
    for p in pulls:
        p.start()
    early, pulls = pulls[:13], pulls[13:]
    early[0].wait()

    rows = tok[...].astype(F32)
    for r in range(2):
        rows_of(tokf, rows[r : r + 1, :], r * 32)
    buf[me] = tall(tokf[...], 2).astype(BF16)
    for p in early[1:]:
        p.wait()
    for conv, taps, dst, n in ((conv_x, conv_x_w, convx, 32), (conv_bc, conv_bc_w, convbc, 8)):
        old = conv[0].astype(F32) * taps[0:1, :]
        for c in range(1, 3):
            old = old + conv[c].astype(F32) * taps[c : c + 1, :]
        for r in range(2):
            rows_of(dst, old[r : r + 1, :], r * n)
        rows_of(dst, taps[3:4, :], 2 * n)
    lane = lax.broadcasted_iota(jnp.int32, (1, LANES), 1)
    dense = jnp.zeros((1, LANES), F32)
    for r in range(2):
        for k in range(TOPK):
            dense = dense + jnp.where(lane == routes[r, k] + 32 * r, weights[r, k], 0.0)
    high = dense.astype(BF16).astype(F32)
    flat[pl.ds(3, 32, stride=8), :] = jnp.broadcast_to(high, (32, LANES))
    flat[pl.ds(7, 32, stride=8), :] = jnp.broadcast_to(dense - high, (32, LANES))
    blank = jnp.zeros((1, 64), F32)

    def column(row):
        return jnp.transpose(jnp.broadcast_to(row, (LANES, LANES)))

    skipbc[...] = column(jnp.concatenate([skip_gain[...], blank], axis=1))
    sq[...] = jnp.zeros((64, LANES), F32)
    ready()

    def staged(source):
        def landed(*blocks):
            for block in blocks:
                both = source[block].astype(F32)
                for r in range(2):
                    stage[pl.ds(pl.multiple_of((block * 2 + r) * PITCH, 8), 32), :] = both[r]

        return landed

    comm.gather_start(buf, send1, recv1)
    comm.gather(buf, send1, recv1, staged(buf))
    for p in pulls[:4]:
        p.wait()
    square = jnp.zeros((64, LANES), F32)
    z, x, st = jnp.zeros((64, LANES), F32), jnp.zeros((64, LANES), F32), jnp.zeros((64, 96), F32)
    for k in range(16):
        part = []
        for j in (2 * k, 2 * k + 1):
            chunk = stage[pl.ds(j, 64, stride=PITCH), :]
            square = square + chunk * chunk
            xraw[:, j * LANES : (j + 1) * LANES] = chunk.astype(BF16)
            part.append((chunk * mix_gain[j : j + 1, :]).astype(BF16))
        part = jnp.concatenate(part, axis=1)
        at = slice(k * 256, (k + 1) * 256)
        z = z + jnp.dot(part, wz[at, :], preferred_element_type=F32)
        x = x + jnp.dot(part, wx[at, :], preferred_element_type=F32)
        st = st + lax.dot_general(part, wst[:, at], (((1,), (1,)), ((), ())), preferred_element_type=F32)
    scale = lax.rsqrt(jnp.sum(square, axis=1, keepdims=True) / 4096.0 + 1e-6)
    z, x, st = z * scale, x * scale, st * scale
    flat[pl.ds(0, 64, stride=4), :] = z
    flat[pl.ds(1, 64, stride=4), :] = x
    bc = st[:, 64:96]
    spread = jnp.concatenate([bc, bc, bc, bc], axis=1)
    flat[pl.ds(2, 64, stride=4), :] = jnp.where(lax.div(lane, 32) == lax.rem(me, 4), spread, 0.0)
    out[...] = tall(flat[...], 32).astype(BF16)
    comm.exchange(out, back, xsend, xrecv)

    flat[pl.ds(0, 64, stride=4), :] = jnp.concatenate([st[:, 0:64], st[:, 0:64]], axis=1)
    mine8 = flat[pl.ds(pl.multiple_of(me * 8, 8), 8), :]
    bias = jnp.concatenate([step_bias[...], blank], axis=1)
    rate = jnp.exp(jnp.concatenate([decay_log[...], blank], axis=1))
    for r in range(2):
        step = jax.nn.softplus(mine8[r * 4 : r * 4 + 1, :] + bias)
        stepbc[pl.ds(r * LANES, LANES), :] = column(step)
        decaybc[pl.ds(r * LANES, LANES), :] = column(jnp.exp(-step * rate))
    low = lax.broadcasted_iota(jnp.int32, (32, LANES), 1) < 64

    def spread_heads(source, base):
        return jnp.where(
            low, source[pl.ds(base, 32, stride=2), :], source[pl.ds(base + 1, 32, stride=2), :]
        )

    gacc[...] = jnp.zeros((64, 1024), F32)
    pulls[4].wait()

    def narrow(i, carry):
        r, g = lax.div(i, 4), lax.rem(i, 4)
        heads = state[r, pl.ds(g * 16, 16)].reshape(1024, LANES)
        narrowed[pl.ds(pl.multiple_of(i * 1024, 1024), 1024), :] = heads.astype(BF16)
        return carry

    lax.fori_loop(0, 8, narrow, 0)
    comm.exchanged(out, back, xsend, xrecv, lambda frm: None)
    flat[...] = back[...].astype(F32).reshape(256, LANES)
    for r in range(2):
        x_pre = flat[pl.ds(4 * r + 1, 32, stride=8), :]
        bc_pre = flat[pl.ds(4 * r + 2, 8, stride=32), :]
        for q in range(1, 4):
            bc_pre = bc_pre + flat[pl.ds(8 * q + 4 * r + 2, 8, stride=32), :]
        xbuf[pl.ds(r * 32, 32), :] = x_pre
        bcs[pl.ds(16 + r * 8, 8), :] = bc_pre
        xc = jax.nn.silu(convx[pl.ds(r * 32, 32), :] + convx[pl.ds(64, 32), :] * x_pre)
        maps = jax.nn.silu(convbc[pl.ds(r * 8, 8), :] + convbc[pl.ds(16, 8), :] * bc_pre)
        bcs[pl.ds(r * 8, 8), :] = maps
        fed = spread_heads(stepbc, r * LANES) * xc
        total[pl.ds(r * 32, 32), :] = fed
        both = jnp.sum(maps[0:4, :] * maps[4:8, :], axis=1, keepdims=True)
        for g in range(4):
            i = r * 4 + g
            y = lax.dot_general(
                jnp.broadcast_to(maps[4 + g : 5 + g, :], (8, LANES)).astype(BF16),
                narrowed[i * 1024 : (i + 1) * 1024, :],
                (((1,), (1,)), ((), ())),
                preferred_element_type=F32,
            )
            for k in range(8):
                ybuf[i * 8 + k : i * 8 + k + 1, :] = y[0:1, k * LANES : (k + 1) * LANES]
        boths = jnp.concatenate([jnp.broadcast_to(both[g : g + 1, :], (8, LANES)) for g in range(4)], axis=0)
        gated = spread_heads(decaybc, r * LANES) * ybuf[pl.ds(r * 32, 32), :] + fed * boths
        gated = gated + spread_heads(skipbc, 0) * xc
        gated = gated * jax.nn.silu(flat[pl.ds(4 * r, 32, stride=8), :])
        mean = jnp.sum(jnp.sum(gated * gated, axis=1, keepdims=True), axis=0, keepdims=True) / 4096.0
        buf2[me, r] = (gated * lax.rsqrt(mean + 1e-6) * inner_gain[...]).astype(BF16)

    def group(i, carry):
        r, g = lax.div(i, 4), lax.rem(i, 4)
        cols = jnp.transpose(total[pl.ds(pl.multiple_of(i * 8, 8), 8), :])
        into = jnp.broadcast_to(bcs[pl.ds(r * 8 + g, 1), :], (LANES, LANES))
        for k in range(8):
            h = g * 16 + 2 * k
            dec = jnp.concatenate(
                [
                    jnp.broadcast_to(decaybc[pl.ds(r * LANES + h, 1), :], (64, LANES)),
                    jnp.broadcast_to(decaybc[pl.ds(r * LANES + h + 1, 1), :], (64, LANES)),
                ],
                axis=0,
            )
            new = dec * state[r, pl.ds(h, 2)].reshape(LANES, LANES)
            new = new + jnp.broadcast_to(cols[:, k : k + 1], (LANES, LANES)) * into
            state[r, pl.ds(h, 2)] = new.reshape(2, 64, LANES)
        return carry

    comm.gather_start(buf2, send2, recv2)
    lax.fori_loop(0, 4, group, 0)
    comm.gather(buf2, send2, recv2, staged(buf2))
    pulls[5].wait()
    cols_out = jnp.zeros((64, LANES), F32)
    for k in range(16):
        part = [stage[pl.ds(j, 64, stride=PITCH), :].astype(BF16) for j in (2 * k, 2 * k + 1)]
        part = jnp.concatenate(part, axis=1)
        cols_out = cols_out + jnp.dot(part, wo[k * 256 : (k + 1) * 256, :], preferred_element_type=F32)
    buf3[me] = cols_out.astype(BF16)

    def landed3(*blocks):
        part, gates, ups = [], [], []
        for block in blocks:
            cols = pl.ds(pl.multiple_of(block * LANES, LANES), LANES)
            resid = (xraw[:, cols].astype(F32) + buf3[block].astype(F32)).astype(BF16).astype(F32)
            sq[...] = sq[...] + resid * resid
            stage[pl.ds(block, 64, stride=PITCH), :] = resid
            part.append((resid * ffn_gain[pl.ds(block, 1), :]).astype(BF16))
            gates.append(wg[cols, :])
            ups.append(wu[cols, :])
        part = jnp.concatenate(part, axis=1)
        for at, w in ((0, gates), (512, ups)):
            at = pl.ds(at, 512)
            gacc[:, at] = gacc[:, at] + jnp.dot(
                part, jnp.concatenate(w, axis=0), preferred_element_type=F32
            )

    comm.gather_start(buf3, send3, recv3)
    lax.fori_loop(4, 8, group, 0)
    pulls[6].wait()
    pulls[7].wait()
    comm.gather(buf3, send3, recv3, landed3)
    scale = lax.rsqrt(jnp.sum(sq[...], axis=1, keepdims=True) / 4096.0 + 1e-6)
    gate, up = gacc[:, 0:512] * scale, gacc[:, 512:1024] * scale
    act[...] = (jax.nn.silu(gate) * up).astype(BF16)
    pulls[8].wait()
    lanes32 = lax.broadcasted_iota(jnp.int32, (32, LANES), 1)
    dense = flat[pl.ds(3, 32, stride=8), :] + flat[pl.ds(7, 32, stride=8), :]
    for r in range(2):
        picked = jnp.sum(jnp.where(lanes32 == me + 32 * r, dense, 0.0), axis=1, keepdims=True)
        wide[pl.ds(r, 32, stride=2), :] = jnp.broadcast_to(picked, (32, LANES))
    weight = jnp.concatenate([wide[...]] * 4, axis=1)

    def expert(half, part):
        at = pl.ds(pl.multiple_of(half * 2048 + part * 512, 512), 512)
        y = jnp.dot(act[...], wd[:, at], preferred_element_type=F32).astype(BF16).astype(F32)
        return y * weight

    swaps = []
    for ch in range(2):
        for k in range(2):
            half_out[ch, :, k * 512 : (k + 1) * 512] = expert(1 - core, 2 * ch + k).astype(BF16)
        swaps.append(
            comm.copy(half_out.at[ch], half_in.at[ch], hsend.at[ch], hrecv.at[ch], comm.partner())
        )
        swaps[ch].start()
    for ch in range(2):
        own = [expert(core, 2 * ch + k) for k in range(2)]
        swaps[ch].wait()
        for j in range(8):
            k, cols = j // 4, slice(j % 4 * LANES, (j % 4 + 1) * LANES)
            total[pl.ds(8 * ch + j, 64, stride=24), :] = own[k][:, cols] + half_in[
                ch, :, j * LANES : (j + 1) * LANES
            ].astype(F32)

        def pack(t, carry, ch=ch):
            for r in range(2):
                at = pl.ds(pl.multiple_of((t * 2 + r) * 24 + 8 * ch, 8), 8)
                send_rows[ch, t, r] = total[at, :].astype(BF16)
            return carry

        lax.fori_loop(0, ep, pack, 0)
        comm.exchange(send_rows.at[ch], got_rows.at[ch], csend.at[ch], crecv.at[ch])
    for r in range(2):
        tokf[pl.ds(r * 32, 32), :] = stage[pl.ds(pl.multiple_of((me * 2 + r) * PITCH, 8), 32), :]
    for r in range(2):
        row_of(rowx, r, xbuf, r * 32, 32)
        row_of(rowbc, r, bcs, 16 + r * 8, 8)
    for old, new, row in ((conv_x, new_x, rowx), (conv_bc, new_bc, rowbc)):
        new[0] = old[1]
        new[1] = old[2]
        new[2] = row[...].astype(BF16)

    for ch in range(2):

        def arrived(frm, ch=ch):
            h = lax.rem(frm, 2)
            for r in range(2):
                at = pl.ds(pl.multiple_of(r * 32 + h * 16 + ch * 8, 8), 8)
                tokf[at, :] = tokf[at, :] + got_rows[ch, frm, r].astype(F32)

        comm.exchanged(send_rows.at[ch], got_rows.at[ch], csend.at[ch], crecv.at[ch], arrived)
    for r in range(2):
        row_of(rowx, r, tokf, r * 32, 32)
    out_ref[...] = rowx[...].astype(BF16)


def layer(ep, *args):
    dma = pltpu.SemaphoreType.DMA
    v = pltpu.VMEM
    local = [v(a.shape[1:] if a.shape[0] == 1 and a.ndim == 3 else a.shape, a.dtype) for a in args]
    local[4:6] = [v((96, 4096), BF16)]
    del local[12]
    local.insert(12, v((8, LANES), F32))
    local[-2:] = [pltpu.SMEM(a.shape, a.dtype) for a in args[-2:]]
    outs = (
        jax.ShapeDtypeStruct((2, 4096), BF16),
        jax.ShapeDtypeStruct(args[13].shape, F32),
        jax.ShapeDtypeStruct(args[11].shape, BF16),
        jax.ShapeDtypeStruct(args[12].shape, BF16),
    )
    results = pl.pallas_call(
        functools.partial(layer_kernel, ep, len(args), len(outs)),
        out_shape=outs,
        in_specs=[hbm()] * len(args),
        out_specs=(vmem(),) * len(outs),
        scratch_shapes=[
            *local,
            v((ep, 2, 32, LANES), BF16), v((ep, 2, 32, LANES), BF16), v((ep, 64, LANES), BF16),
            v((64 * PITCH, LANES), F32), v((8192, LANES), BF16), v((64, 1024), F32), v((64, 4096), BF16),
            v((256, LANES), F32), v((ep, 8, LANES), BF16), v((ep, 8, LANES), BF16), v((64, LANES), F32),
            v((96, LANES), F32), v((24, LANES), F32),
            v((256, LANES), F32), v((256, LANES), F32), v((LANES, LANES), F32), v((32, LANES), F32),
            v((64, LANES), F32), v((64, LANES), F32), v((2, 4096), F32), v((2, 1024), F32), v((64, LANES), F32),
            v((64, 512), BF16), v((64, LANES), F32), v((2, 64, 1024), BF16), v((2, 64, 1024), BF16),
            v((64 * 24, LANES), F32),
            v((2, ep, 2, 8, LANES), BF16), v((2, ep, 2, 8, LANES), BF16),
            dma((22,)), dma, dma((ep,)), dma, dma((ep,)), dma, dma((ep,)), dma((2,)), dma((2,)), dma, dma((ep,)),
            dma((2,)), dma((2, ep)),
        ],
        compiler_params=pltpu.CompilerParams(
            collective_id=0, has_side_effects=True, vmem_limit_bytes=VMEM_LIMIT
        ),
        name="layer",
    )(*(pltpu.with_memory_space_constraint(a, pltpu.HBM) for a in args))
    return pl.pallas_call(
        flush_kernel,
        out_shape=outs,
        in_specs=[vmem()] * len(outs),
        out_specs=(hbm(),) * len(outs),
        scratch_shapes=[dma((len(outs),))],
        compiler_params=pltpu.CompilerParams(vmem_limit_bytes=1024 * 1024),
        name="flush",
    )(*results)


def flush_kernel(*refs):
    n = len(refs) // 2
    copies = [pltpu.make_async_copy(refs[i], refs[n + i], refs[-1].at[i]) for i in range(n)]
    for c in copies:
        c.start()
    for c in copies:
        c.wait()


def body(
    ep, tokens_in, mix_gain, w_gate_z, w_value, w_in_bc, w_step, step_bias, decay_log, skip_gain, conv_x_weight,
    conv_bc_weight, conv_x_state, conv_bc_state, ssm_state, inner_gain, out_weight, ffn_gain, expert_gate,
    expert_up, expert_down, routes, route_weight,
):
    out, new_state, new_x, new_bc = layer(
        ep, tokens_in, mix_gain.reshape(32, LANES), w_gate_z, w_value, w_in_bc.T, w_step.T,
        step_bias.reshape(1, 64), decay_log.reshape(1, 64), skip_gain.reshape(1, 64), conv_x_weight,
        conv_bc_weight, conv_x_state.transpose(1, 0, 2), conv_bc_state.transpose(1, 0, 2), ssm_state,
        inner_gain.reshape(32, LANES), out_weight, ffn_gain.reshape(32, LANES), expert_gate, expert_up,
        expert_down, routes, route_weight,
    )
    return out, new_state, new_x.transpose(1, 0, 2), new_bc.transpose(1, 0, 2)


def solution(mesh):
    ep = mesh.shape["ep"]
    cols, rep = P(None, "ep"), P()
    placed = (
        P(GRP_EP, None), rep, cols, cols, cols, rep, rep, rep, rep, rep, rep,
        P(GRP_EP, None, None), P(GRP_EP, None, None), P(GRP_EP, None, None, None),
        rep, cols, rep, P("ep", None, None), P("ep", None, None), P("ep", None, None),
        P(GRP_EP, None), P(GRP_EP, None),
    )
    return jax.shard_map(
        functools.partial(body, ep),
        mesh=mesh,
        in_specs=placed,
        out_specs=(
            P(GRP_EP, None),
            P(GRP_EP, None, None, None),
            P(GRP_EP, None, None),
            P(GRP_EP, None, None),
        ),
        check_vma=False,
    )
```

```python
import functools

import jax
import jax.numpy as jnp
from jax import lax
from jax.experimental import pallas as pl
from jax.experimental.pallas import tpu as pltpu
from jax.sharding import PartitionSpec as P

TOPK = 4
GRP_EP = ("grp", "ep")
MESH = pl.DeviceIdType.MESH
F32 = jnp.float32
BF16 = jnp.bfloat16
LANES = 128
PITCH = 40
VMEM_LIMIT = 38 * 1024 * 1024

OWN = (6, -6, 3, -3, 1, -1)
RELAYS = ((3, (1, -1)), (-3, (1, -1)), (6, (2, 1, -1)), (-6, (1, -1)))
GREET = (1, -1, 2, -2, 3, -3, 6, -6)
GROUPS = ((3, -3), (6, -6, 1, -1), (2, -2, 4, -4), (5, -5, 7, -7, 8))


def turned(d, side):
    return d if side == 0 else -d


class Comm:
    def __init__(self, ep):
        self.ep = ep
        self.nz = ep // 2
        self.me = lax.axis_index("ep")
        self.core = lax.rem(self.me, 2)
        self.z = lax.div(self.me, 2)

    def at(self, offset, core):
        return lax.rem(self.z + offset + self.nz, self.nz) * 2 + core

    def partner(self):
        return self.z * 2 + (1 - self.core)

    def barrier(self):
        sem = pltpu.get_barrier_semaphore()

        def greet(to):
            pl.semaphore_signal(sem, inc=1, device_id={"ep": to}, device_id_type=MESH)

        @pl.when(self.core == 1)
        def _():
            for d in GREET:
                greet(self.at(d, 0))
                greet(self.at(d, 1))

        greet(self.partner())
        return lambda: pl.semaphore_wait(sem, len(GREET) + 1)

    def copy(self, src, dst, send, recv, to):
        return pltpu.make_async_remote_copy(
            src_ref=src, dst_ref=dst, send_sem=send, recv_sem=recv, device_id={"ep": to}, device_id_type=MESH
        )

    def gather_start(self, buf, send, recv):
        me = self.me
        for to in [self.at(d * (1 - 2 * self.core), 1) for d in OWN] + [self.partner()]:
            self.copy(buf.at[me], buf.at[me], send, recv.at[me], to).start()

    def gather(self, buf, send, recv, landed):
        core, me = self.core, self.me

        def pass_on(block, to):
            self.copy(buf.at[block], buf.at[block], send, recv.at[block], to).start()

        def arrive(block):
            self.copy(buf.at[block], buf.at[block], send, recv.at[block], me).wait_recv()

        def sent(n):
            whole = buf.at[pl.ds(0, n)]
            self.copy(whole, whole, send, recv.at[0], me).wait_send()

        relays = dict(RELAYS)

        @pl.when(core == 1)
        def _():
            arrive(self.partner())
            blocks, passed = [me, self.partner()], 0
            for offsets in GROUPS:
                for d in offsets:
                    for side in range(2):
                        block = self.at(-turned(d, side), side)
                        arrive(block)
                        for step in relays.get(d, ()):
                            pass_on(block, self.at(turned(step, side), 1))
                            passed += 1
                        pass_on(block, self.partner())
                        passed += 1
                        blocks.append(block)
                landed(blocks)
                blocks = []
            sent(len(OWN) + 1)
            for start in range(0, passed, self.ep):
                sent(min(self.ep, passed - start))

        @pl.when(core == 0)
        def _():
            arrive(self.partner())
            blocks = [me, self.partner()]
            for offsets in GROUPS:
                for d in offsets:
                    for side in range(2):
                        block = self.at(-turned(d, side), side)
                        arrive(block)
                        blocks.append(block)
                landed(blocks)
                blocks = []
            sent(len(OWN) + 1)

    def reduce(self, own, parts, relay_in, relay_out, final_in, sums, send, relay_sem, final_sem):
        core, me = self.core, self.me
        slots = {(d, step): i for i, (d, step) in enumerate((d, step) for d, on in RELAYS for step in on)}
        finals = {d: i for i, d in enumerate(OWN)}
        relays = [d for d, _ in RELAYS]
        per = len(slots)

        def leaf(d, step, side):
            slot = side * per + slots[d, step]
            to = self.at(-turned(step, side), core)
            part = parts.at[self.at(-turned(d + step, side), side)]
            return self.copy(part, relay_in.at[slot], send, relay_sem.at[slot], to)

        def final(d, side, source):
            slot = side * len(OWN) + finals[d]
            return self.copy(source, final_in.at[slot], send, final_sem.at[slot], self.at(-turned(d, side), core))

        for d, onward in reversed(RELAYS):
            for step in onward:
                for side in range(2):
                    leaf(d, step, side).start()
        for d in OWN:
            if d not in relays:
                for side in range(2):
                    final(d, side, parts.at[self.at(-turned(d, side), side)]).start()
        for d, onward in reversed(RELAYS):
            for side in range(2):
                total = own(self.at(-turned(d, side), side))
                for step in onward:
                    slot = side * per + slots[d, step]
                    leaf(d, step, side).wait_recv()
                    total = total + relay_in[slot].astype(F32)
                at = side * len(relays) + relays.index(d)
                relay_out[at] = total.astype(BF16)
                final(d, side, relay_out.at[at]).start()
        for side in range(2):
            sums[side] = own(self.z * 2 + side)
        for d in reversed(OWN):
            for side in range(2):
                final(d, side, relay_out.at[0]).wait_recv()
                sums[side] = sums[side] + final_in[side * len(OWN) + finals[d]].astype(F32)
        whole = parts.at[pl.ds(0, 2 * (per + len(OWN)))]
        self.copy(whole, whole, send, final_sem.at[0], me).wait_send()

    def exchange(self, out, back, send, recv):
        me, ep, nz = self.me, self.ep, self.nz

        def one(to):
            self.copy(out.at[to], back.at[me], send, recv.at[me], to).start()

        def far_first(k, carry):
            offset = (nz // 2 - lax.div(k + 1, 2)) * (1 - 2 * lax.rem(k, 2))
            one(self.at(offset, 0))
            one(self.at(offset, 1))
            return carry

        lax.fori_loop(0, nz - 1, far_first, 0)
        one(self.partner())
        back[me] = out[me]

    def exchanged(self, out, back, send, recv, landed):
        me, ep = self.me, self.ep
        landed(me)

        def one(i, carry):
            frm = lax.rem(me + i, ep)
            self.copy(back.at[frm], back.at[frm], send, recv.at[frm], me).wait_recv()
            landed(frm)
            return carry

        lax.fori_loop(1, ep, one, 0)
        whole = out.at[pl.ds(0, ep - 1)]
        self.copy(whole, whole, send, recv.at[0], me).wait_send()


def tall(x, n):
    return x.reshape(n, x.shape[0] // n, x.shape[1])


def vmem():
    return pl.BlockSpec(memory_space=pltpu.VMEM)


def hbm():
    return pl.BlockSpec(memory_space=pl.ANY)


def smem():
    return pl.BlockSpec(memory_space=pltpu.SMEM)


def rows_of(dst, src, base):
    for j in range(src.shape[1] // LANES):
        dst[base + j : base + j + 1, :] = src[:, j * LANES : (j + 1) * LANES]


def row_of(dst, r, src, base, n):
    for j in range(n):
        dst[r : r + 1, j * LANES : (j + 1) * LANES] = src[base + j : base + j + 1, :]


def layer_kernel(ep, n_in, n_out, *refs):
    inputs, outputs, locals_, refs = (
        refs[:n_in], refs[n_in : n_in + n_out], refs[n_in + n_out : 2 * n_in + n_out - 1], refs[2 * n_in + n_out - 1 :]
    )
    (
        tok, mix_gain, wz, wx, wst, step_bias, decay_log, skip_gain, conv_x_w, conv_bc_w, conv_x, conv_bc, _,
        inner_gain, wo, ffn_gain, wg, wu, wd, routes, weights,
    ) = locals_
    out_ref, state, new_x, new_bc = outputs
    (
        buf, buf2, buf3, stage, narrowed, gacc, xraw, flat, out, back, tokf, convx, convbc,
        stepbc, decaybc, skipbc, bcs, ybuf, xbuf, rowx, rowbc, sq, act, wide, half_out, half_in, total,
        send_rows, relay_in, relay_out, final_in, sums, handed,
        wload, send1, recv1, send2, recv2, send3, recv3, hsend, hrecv, xsend, xrecv, csend, relay_sem, final_sem, fsend, frecv,
    ) = refs
    comm = Comm(ep)
    me, core = comm.me, comm.core
    ready = comm.barrier()
    (
        tok_h, mix_h, wz_h, wx_h, wbc_h, wst_h, bias_h, decay_h, skip_h, cxw_h, cbw_h, cx_h, cb_h, state_h, inner_h,
        wo_h, ffn_h, wg_h, wu_h, wd_h, routes_h, weights_h,
    ) = inputs
    pairs = (
        (tok_h, tok), (cx_h, conv_x), (cxw_h, conv_x_w), (cb_h, conv_bc), (cbw_h, conv_bc_w), (routes_h, routes),
        (weights_h, weights), (skip_h, skip_gain), (bias_h, step_bias), (decay_h, decay_log), (mix_h, mix_gain),
        (inner_h, inner_gain), (ffn_h, ffn_gain),
        (wz_h, wz), (wx_h, wx), (wst_h, wst.at[pl.ds(0, 64)]), (wbc_h, wst.at[pl.ds(64, 32)]),
        (state_h, state), (wo_h, wo), (wg_h.at[0], wg), (wu_h.at[0], wu), (wd_h.at[0], wd),
    )
    pulls = [pltpu.make_async_copy(a, b, wload.at[i]) for i, (a, b) in enumerate(pairs)]
    for p in pulls:
        p.start()
    early, pulls = pulls[:13], pulls[13:]
    early[0].wait()

    rows = tok[...].astype(F32)
    for r in range(2):
        rows_of(tokf, rows[r : r + 1, :], r * 32)
    buf[me] = tall(tokf[...], 2).astype(BF16)
    ready()
    comm.gather_start(buf, send1, recv1)
    for p in early[1:]:
        p.wait()
    for conv, taps, dst, n in ((conv_x, conv_x_w, convx, 32), (conv_bc, conv_bc_w, convbc, 8)):
        old = conv[0].astype(F32) * taps[0:1, :]
        for c in range(1, 3):
            old = old + conv[c].astype(F32) * taps[c : c + 1, :]
        for r in range(2):
            rows_of(dst, old[r : r + 1, :], r * n)
        rows_of(dst, taps[3:4, :], 2 * n)
    lane = lax.broadcasted_iota(jnp.int32, (1, LANES), 1)
    dense = jnp.zeros((1, LANES), F32)
    for r in range(2):
        for k in range(TOPK):
            dense = dense + jnp.where(lane == routes[r, k] + 32 * r, weights[r, k], 0.0)
    high = dense.astype(BF16).astype(F32)
    flat[pl.ds(3, 32, stride=8), :] = jnp.broadcast_to(high, (32, LANES))
    flat[pl.ds(7, 32, stride=8), :] = jnp.broadcast_to(dense - high, (32, LANES))
    blank = jnp.zeros((1, 64), F32)

    def column(row):
        return jnp.transpose(jnp.broadcast_to(row, (LANES, LANES)))

    skipbc[...] = column(jnp.concatenate([skip_gain[...], blank], axis=1))
    sq[...] = jnp.zeros((64, LANES), F32)

    def staged(source):
        def landed(blocks):
            for block in blocks:
                both = source[block].astype(F32)
                for r in range(2):
                    stage[pl.ds(pl.multiple_of((block * 2 + r) * PITCH, 8), 32), :] = both[r]

        return landed

    comm.gather(buf, send1, recv1, staged(buf))
    for p in pulls[:4]:
        p.wait()
    square = jnp.zeros((64, LANES), F32)
    z, x, st = jnp.zeros((64, LANES), F32), jnp.zeros((64, LANES), F32), jnp.zeros((64, 96), F32)
    for k in range(16):
        part = []
        for j in (2 * k, 2 * k + 1):
            chunk = stage[pl.ds(j, 64, stride=PITCH), :]
            square = square + chunk * chunk
            xraw[:, j * LANES : (j + 1) * LANES] = chunk.astype(BF16)
            part.append((chunk * mix_gain[j : j + 1, :]).astype(BF16))
        part = jnp.concatenate(part, axis=1)
        at = slice(k * 256, (k + 1) * 256)
        z = z + jnp.dot(part, wz[at, :], preferred_element_type=F32)
        x = x + jnp.dot(part, wx[at, :], preferred_element_type=F32)
        st = st + lax.dot_general(part, wst[:, at], (((1,), (1,)), ((), ())), preferred_element_type=F32)
    scale = lax.rsqrt(jnp.sum(square, axis=1, keepdims=True) / 4096.0 + 1e-6)
    z, x, st = z * scale, x * scale, st * scale
    flat[pl.ds(0, 64, stride=4), :] = z
    flat[pl.ds(1, 64, stride=4), :] = x
    bc = st[:, 64:96]
    spread = jnp.concatenate([bc, bc, bc, bc], axis=1)
    flat[pl.ds(2, 64, stride=4), :] = jnp.where(lax.div(lane, 32) == lax.rem(me, 4), spread, 0.0)
    out[...] = tall(flat[...], 32).astype(BF16)
    comm.exchange(out, back, xsend, xrecv)

    flat[pl.ds(0, 64, stride=4), :] = jnp.concatenate([st[:, 0:64], st[:, 0:64]], axis=1)
    mine8 = flat[pl.ds(pl.multiple_of(me * 8, 8), 8), :]
    bias = jnp.concatenate([step_bias[...], blank], axis=1)
    rate = jnp.exp(jnp.concatenate([decay_log[...], blank], axis=1))
    for r in range(2):
        step = jax.nn.softplus(mine8[r * 4 : r * 4 + 1, :] + bias)
        stepbc[pl.ds(r * LANES, LANES), :] = column(step)
        decaybc[pl.ds(r * LANES, LANES), :] = column(jnp.exp(-step * rate))
    low = lax.broadcasted_iota(jnp.int32, (32, LANES), 1) < 64

    def spread_heads(source, base):
        return jnp.where(
            low, source[pl.ds(base, 32, stride=2), :], source[pl.ds(base + 1, 32, stride=2), :]
        )

    gacc[...] = jnp.zeros((64, 1024), F32)
    pulls[4].wait()

    def narrow(i, carry):
        r, g = lax.div(i, 4), lax.rem(i, 4)
        heads = state[r, pl.ds(g * 16, 16)].reshape(1024, LANES)
        narrowed[pl.ds(pl.multiple_of(i * 1024, 1024), 1024), :] = heads.astype(BF16)
        return carry

    lax.fori_loop(0, 8, narrow, 0)
    comm.exchanged(out, back, xsend, xrecv, lambda frm: None)
    flat[...] = back[...].astype(F32).reshape(256, LANES)
    for r in range(2):
        x_pre = flat[pl.ds(4 * r + 1, 32, stride=8), :]
        bc_pre = flat[pl.ds(4 * r + 2, 8, stride=32), :]
        for q in range(1, 4):
            bc_pre = bc_pre + flat[pl.ds(8 * q + 4 * r + 2, 8, stride=32), :]
        xbuf[pl.ds(r * 32, 32), :] = x_pre
        bcs[pl.ds(16 + r * 8, 8), :] = bc_pre
        xc = jax.nn.silu(convx[pl.ds(r * 32, 32), :] + convx[pl.ds(64, 32), :] * x_pre)
        maps = jax.nn.silu(convbc[pl.ds(r * 8, 8), :] + convbc[pl.ds(16, 8), :] * bc_pre)
        bcs[pl.ds(r * 8, 8), :] = maps
        fed = spread_heads(stepbc, r * LANES) * xc
        total[pl.ds(r * 32, 32), :] = fed
        both = jnp.sum(maps[0:4, :] * maps[4:8, :], axis=1, keepdims=True)
        for g in range(4):
            i = r * 4 + g
            y = lax.dot_general(
                jnp.broadcast_to(maps[4 + g : 5 + g, :], (8, LANES)).astype(BF16),
                narrowed[i * 1024 : (i + 1) * 1024, :],
                (((1,), (1,)), ((), ())),
                preferred_element_type=F32,
            )
            for k in range(8):
                ybuf[i * 8 + k : i * 8 + k + 1, :] = y[0:1, k * LANES : (k + 1) * LANES]
        boths = jnp.concatenate([jnp.broadcast_to(both[g : g + 1, :], (8, LANES)) for g in range(4)], axis=0)
        gated = spread_heads(decaybc, r * LANES) * ybuf[pl.ds(r * 32, 32), :] + fed * boths
        gated = gated + spread_heads(skipbc, 0) * xc
        gated = gated * jax.nn.silu(flat[pl.ds(4 * r, 32, stride=8), :])
        mean = jnp.sum(jnp.sum(gated * gated, axis=1, keepdims=True), axis=0, keepdims=True) / 4096.0
        buf2[me, r] = (gated * lax.rsqrt(mean + 1e-6) * inner_gain[...]).astype(BF16)

    def group(i, carry):
        r, g = lax.div(i, 4), lax.rem(i, 4)
        cols = jnp.transpose(total[pl.ds(pl.multiple_of(i * 8, 8), 8), :])
        into = jnp.broadcast_to(bcs[pl.ds(r * 8 + g, 1), :], (LANES, LANES))
        for k in range(8):
            h = g * 16 + 2 * k
            dec = jnp.concatenate(
                [
                    jnp.broadcast_to(decaybc[pl.ds(r * LANES + h, 1), :], (64, LANES)),
                    jnp.broadcast_to(decaybc[pl.ds(r * LANES + h + 1, 1), :], (64, LANES)),
                ],
                axis=0,
            )
            new = dec * state[r, pl.ds(h, 2)].reshape(LANES, LANES)
            new = new + jnp.broadcast_to(cols[:, k : k + 1], (LANES, LANES)) * into
            state[r, pl.ds(h, 2)] = new.reshape(2, 64, LANES)
        return carry

    comm.gather_start(buf2, send2, recv2)
    lax.fori_loop(0, 4, group, 0)
    comm.gather(buf2, send2, recv2, staged(buf2))
    pulls[5].wait()
    cols_out = jnp.zeros((64, LANES), F32)
    for k in range(16):
        part = [stage[pl.ds(j, 64, stride=PITCH), :].astype(BF16) for j in (2 * k, 2 * k + 1)]
        part = jnp.concatenate(part, axis=1)
        cols_out = cols_out + jnp.dot(part, wo[k * 256 : (k + 1) * 256, :], preferred_element_type=F32)
    buf3[me] = cols_out.astype(BF16)

    def landed3(blocks):
        gates, ups, square = gacc[:, 0:512], gacc[:, 512:1024], sq[...]
        for pair in zip(blocks[::2], blocks[1::2], strict=True):
            part, gate_rows, up_rows = [], [], []
            for block in pair:
                cols = pl.ds(pl.multiple_of(block * LANES, LANES), LANES)
                resid = (xraw[:, cols].astype(F32) + buf3[block].astype(F32)).astype(BF16).astype(F32)
                square = square + resid * resid
                stage[pl.ds(block, 64, stride=PITCH), :] = resid
                part.append((resid * ffn_gain[pl.ds(block, 1), :]).astype(BF16))
                gate_rows.append(wg[cols, :])
                up_rows.append(wu[cols, :])
            part = jnp.concatenate(part, axis=1)
            gates = gates + jnp.dot(part, jnp.concatenate(gate_rows, axis=0), preferred_element_type=F32)
            ups = ups + jnp.dot(part, jnp.concatenate(up_rows, axis=0), preferred_element_type=F32)
        gacc[:, 0:512], gacc[:, 512:1024], sq[...] = gates, ups, square

    comm.gather_start(buf3, send3, recv3)
    lax.fori_loop(4, 8, group, 0)
    pulls[6].wait()
    pulls[7].wait()
    comm.gather(buf3, send3, recv3, landed3)
    scale = lax.rsqrt(jnp.sum(sq[...], axis=1, keepdims=True) / 4096.0 + 1e-6)
    gate, up = gacc[:, 0:512] * scale, gacc[:, 512:1024] * scale
    act[...] = (jax.nn.silu(gate) * up).astype(BF16)
    pulls[8].wait()
    lanes32 = lax.broadcasted_iota(jnp.int32, (32, LANES), 1)
    dense = flat[pl.ds(3, 32, stride=8), :] + flat[pl.ds(7, 32, stride=8), :]
    for r in range(2):
        picked = jnp.sum(jnp.where(lanes32 == me + 32 * r, dense, 0.0), axis=1, keepdims=True)
        wide[pl.ds(r, 32, stride=2), :] = jnp.broadcast_to(picked, (32, LANES))
    weight = jnp.concatenate([wide[...]] * 4, axis=1)

    def expert(half, part):
        at = pl.ds(pl.multiple_of(half * 2048 + part * 512, 512), 512)
        y = jnp.dot(act[...], wd[:, at], preferred_element_type=F32).astype(BF16).astype(F32)
        return y * weight

    swaps = []
    for ch in range(2):
        for k in range(2):
            half_out[ch, :, k * 512 : (k + 1) * 512] = expert(1 - core, 2 * ch + k).astype(BF16)
        swaps.append(
            comm.copy(half_out.at[ch], half_in.at[ch], hsend.at[ch], hrecv.at[ch], comm.partner())
        )
        swaps[ch].start()
    for ch in range(2):
        own = [expert(core, 2 * ch + k) for k in range(2)]
        swaps[ch].wait()
        for j in range(8):
            k, cols = j // 4, slice(j % 4 * LANES, (j % 4 + 1) * LANES)
            total[pl.ds(8 * ch + j, 64, stride=24), :] = own[k][:, cols] + half_in[
                ch, :, j * LANES : (j + 1) * LANES
            ].astype(F32)


    def pack(t, carry):
        for r in range(2):
            send_rows[t, r] = total[pl.ds(pl.multiple_of((t * 2 + r) * 24, 8), 16), :].astype(BF16)
        return carry

    lax.fori_loop(0, ep, pack, 0)

    def chip_rows(device):
        at = [pl.ds(pl.multiple_of((device * 2 + r) * 24, 8), 16) for r in range(2)]
        return jnp.stack([total[a, :] for a in at])

    comm.reduce(chip_rows, send_rows, relay_in, relay_out, final_in, sums, csend, relay_sem, final_sem)
    hand = comm.copy(sums.at[1 - core], handed, fsend, frecv, comm.partner())
    hand.start()
    for r in range(2):
        tokf[pl.ds(r * 32, 32), :] = stage[pl.ds(pl.multiple_of((me * 2 + r) * PITCH, 8), 32), :]
    for r in range(2):
        row_of(rowx, r, xbuf, r * 32, 32)
        row_of(rowbc, r, bcs, 16 + r * 8, 8)
    for old, new, row in ((conv_x, new_x, rowx), (conv_bc, new_bc, rowbc)):
        new[0] = old[1]
        new[1] = old[2]
        new[2] = row[...].astype(BF16)

    hand.wait()
    for half, source in ((core, sums.at[core]), (1 - core, handed)):
        for r in range(2):
            at = pl.ds(pl.multiple_of(r * 32 + half * 16, 8), 16)
            tokf[at, :] = tokf[at, :] + source[r]
    for r in range(2):
        row_of(rowx, r, tokf, r * 32, 32)
    out_ref[...] = rowx[...].astype(BF16)


def layer(ep, *args):
    dma = pltpu.SemaphoreType.DMA
    v = pltpu.VMEM
    local = [v(a.shape[1:] if a.shape[0] == 1 and a.ndim == 3 else a.shape, a.dtype) for a in args]
    local[4:6] = [v((96, 4096), BF16)]
    del local[12]
    local.insert(12, v((8, LANES), F32))
    local[-2:] = [pltpu.SMEM(a.shape, a.dtype) for a in args[-2:]]
    outs = (
        jax.ShapeDtypeStruct((2, 4096), BF16),
        jax.ShapeDtypeStruct(args[13].shape, F32),
        jax.ShapeDtypeStruct(args[11].shape, BF16),
        jax.ShapeDtypeStruct(args[12].shape, BF16),
    )
    results = pl.pallas_call(
        functools.partial(layer_kernel, ep, len(args), len(outs)),
        out_shape=outs,
        in_specs=[hbm()] * len(args),
        out_specs=(vmem(),) * len(outs),
        scratch_shapes=[
            *local,
            v((ep, 2, 32, LANES), BF16), v((ep, 2, 32, LANES), BF16), v((ep, 64, LANES), BF16),
            v((64 * PITCH, LANES), F32), v((8192, LANES), BF16), v((64, 1024), F32), v((64, 4096), BF16),
            v((256, LANES), F32), v((ep, 8, LANES), BF16), v((ep, 8, LANES), BF16), v((64, LANES), F32),
            v((96, LANES), F32), v((24, LANES), F32),
            v((256, LANES), F32), v((256, LANES), F32), v((LANES, LANES), F32), v((32, LANES), F32),
            v((64, LANES), F32), v((64, LANES), F32), v((2, 4096), F32), v((2, 1024), F32), v((64, LANES), F32),
            v((64, 512), BF16), v((64, LANES), F32), v((2, 64, 1024), BF16), v((2, 64, 1024), BF16),
            v((64 * 24, LANES), F32),
            v((ep, 2, 16, LANES), BF16), v((18, 2, 16, LANES), BF16), v((8, 2, 16, LANES), BF16),
            v((12, 2, 16, LANES), BF16), v((2, 2, 16, LANES), F32), v((2, 16, LANES), F32),
            dma((22,)), dma, dma((ep,)), dma, dma((ep,)), dma, dma((ep,)), dma((2,)), dma((2,)), dma, dma((ep,)),
            dma, dma((18,)), dma((12,)), dma, dma,
        ],
        compiler_params=pltpu.CompilerParams(
            collective_id=0, has_side_effects=True, vmem_limit_bytes=VMEM_LIMIT
        ),
        name="layer",
    )(*(pltpu.with_memory_space_constraint(a, pltpu.HBM) for a in args))
    return pl.pallas_call(
        flush_kernel,
        out_shape=outs,
        in_specs=[vmem()] * len(outs),
        out_specs=(hbm(),) * len(outs),
        scratch_shapes=[dma((len(outs),))],
        compiler_params=pltpu.CompilerParams(vmem_limit_bytes=1024 * 1024),
        name="flush",
    )(*results)


def flush_kernel(*refs):
    n = len(refs) // 2
    copies = [pltpu.make_async_copy(refs[i], refs[n + i], refs[-1].at[i]) for i in range(n)]
    for c in copies:
        c.start()
    for c in copies:
        c.wait()


def body(
    ep, tokens_in, mix_gain, w_gate_z, w_value, w_in_bc, w_step, step_bias, decay_log, skip_gain, conv_x_weight,
    conv_bc_weight, conv_x_state, conv_bc_state, ssm_state, inner_gain, out_weight, ffn_gain, expert_gate,
    expert_up, expert_down, routes, route_weight,
):
    out, new_state, new_x, new_bc = layer(
        ep, tokens_in, mix_gain.reshape(32, LANES), w_gate_z, w_value, w_in_bc.T, w_step.T,
        step_bias.reshape(1, 64), decay_log.reshape(1, 64), skip_gain.reshape(1, 64), conv_x_weight,
        conv_bc_weight, conv_x_state.transpose(1, 0, 2), conv_bc_state.transpose(1, 0, 2), ssm_state,
        inner_gain.reshape(32, LANES), out_weight, ffn_gain.reshape(32, LANES), expert_gate, expert_up,
        expert_down, routes, route_weight,
    )
    return out, new_state, new_x.transpose(1, 0, 2), new_bc.transpose(1, 0, 2)


def solution(mesh):
    ep = mesh.shape["ep"]
    cols, rep = P(None, "ep"), P()
    placed = (
        P(GRP_EP, None), rep, cols, cols, cols, rep, rep, rep, rep, rep, rep,
        P(GRP_EP, None, None), P(GRP_EP, None, None), P(GRP_EP, None, None, None),
        rep, cols, rep, P("ep", None, None), P("ep", None, None), P("ep", None, None),
        P(GRP_EP, None), P(GRP_EP, None),
    )
    return jax.shard_map(
        functools.partial(body, ep),
        mesh=mesh,
        in_specs=placed,
        out_specs=(
            P(GRP_EP, None),
            P(GRP_EP, None, None, None),
            P(GRP_EP, None, None),
            P(GRP_EP, None, None),
        ),
        check_vma=False,
    )
```

```python
import functools

import jax
import jax.numpy as jnp
from jax import lax
from jax.experimental import pallas as pl
from jax.experimental.pallas import tpu as pltpu
from jax.sharding import PartitionSpec as P

TOPK = 4
GRP_EP = ("grp", "ep")
MESH = pl.DeviceIdType.MESH
F32 = jnp.float32
BF16 = jnp.bfloat16
LANES = 128
PITCH = 40
VMEM_LIMIT = 38 * 1024 * 1024

OWN = (6, -6, 3, -3, 1, -1)
RELAYS = ((3, (1, -1)), (-3, (1, -1)), (6, (2, 1, -1)), (-6, (1, -1)))
OWN_FIRST = (3, -3, 1, -1)
RELAYS_FIRST = ((3, (3, 1, -1)), (-3, (-3, 1, -1)), (6, (2, 1, -1)), (-6, (1, -1)))
GREET = (1, -1, 2, -2, 3, -3)
GROUPS = ((3, -3), (6, -6, 1, -1), (2, -2, 4, -4, 5, -5), (7, -7, 8))


def turned(d, side):
    return d if side == 0 else -d


class Comm:
    def __init__(self, ep):
        self.ep = ep
        self.nz = ep // 2
        self.me = lax.axis_index("ep")
        self.core = lax.rem(self.me, 2)
        self.z = lax.div(self.me, 2)

    def at(self, offset, core):
        return lax.rem(self.z + offset + self.nz, self.nz) * 2 + core

    def partner(self):
        return self.z * 2 + (1 - self.core)

    def barrier(self):
        sem = pltpu.get_barrier_semaphore()

        def greet(to):
            pl.semaphore_signal(sem, inc=1, device_id={"ep": to}, device_id_type=MESH)

        @pl.when(self.core == 1)
        def _():
            for d in GREET:
                greet(self.at(d, 0))
                greet(self.at(d, 1))

        greet(self.partner())
        return lambda: pl.semaphore_wait(sem, len(GREET) + 1)

    def copy(self, src, dst, send, recv, to):
        return pltpu.make_async_remote_copy(
            src_ref=src, dst_ref=dst, send_sem=send, recv_sem=recv, device_id={"ep": to}, device_id_type=MESH
        )

    def gather_start(self, buf, send, recv, own=OWN):
        me = self.me
        for to in [self.at(d * (1 - 2 * self.core), 1) for d in own] + [self.partner()]:
            self.copy(buf.at[me], buf.at[me], send, recv.at[me], to).start()

    def gather(self, buf, send, recv, landed, own=OWN, onward=RELAYS):
        core, me = self.core, self.me

        def pass_on(block, to):
            self.copy(buf.at[block], buf.at[block], send, recv.at[block], to).start()

        def arrive(block):
            self.copy(buf.at[block], buf.at[block], send, recv.at[block], me).wait_recv()

        def sent(n):
            whole = buf.at[pl.ds(0, n)]
            self.copy(whole, whole, send, recv.at[0], me).wait_send()

        relays = dict(onward)

        @pl.when(core == 1)
        def _():
            arrive(self.partner())
            blocks, passed = [me, self.partner()], 0
            for offsets in GROUPS:
                for d in offsets:
                    for side in range(2):
                        block = self.at(-turned(d, side), side)
                        arrive(block)
                        for step in relays.get(d, ()):
                            pass_on(block, self.at(turned(step, side), 1))
                            passed += 1
                        pass_on(block, self.partner())
                        passed += 1
                        blocks.append(block)
                if offsets == GROUPS[-2]:
                    continue
                landed(blocks)
                blocks = []
            sent(len(own) + 1)
            for start in range(0, passed, self.ep):
                sent(min(self.ep, passed - start))

        @pl.when(core == 0)
        def _():
            arrive(self.partner())
            blocks = [me, self.partner()]
            for offsets in GROUPS:
                for d in offsets:
                    for side in range(2):
                        block = self.at(-turned(d, side), side)
                        arrive(block)
                        blocks.append(block)
                landed(blocks)
                blocks = []
            sent(len(own) + 1)

    def reduce(self, own, parts, relay_in, relay_out, final_in, sums, send, relay_sem, final_sem):
        core, me = self.core, self.me
        slots = {(d, step): i for i, (d, step) in enumerate((d, step) for d, on in RELAYS for step in on)}
        relays = [d for d, _ in RELAYS]
        per, ends = len(slots), len(OWN) + 1

        def leaf(d, step, side):
            slot = side * per + slots[d, step]
            to = self.at(-turned(step, side), core)
            part = parts.at[self.at(-turned(d + step, side), side)]
            return self.copy(part, relay_in.at[slot], send, relay_sem.at[slot], to)

        def final(i, half, source, to):
            slot = half * ends + i
            return self.copy(source, final_in.at[slot], send, final_sem.at[slot], to)

        for d, onward in reversed(RELAYS):
            for step in onward:
                for side in range(2):
                    leaf(d, step, side).start()
        for i, d in enumerate(OWN):
            if d not in relays:
                for side in range(2):
                    to = self.at(-turned(d, side), side)
                    final(i, core, parts.at[to], to).start()
        final(ends - 1, core, parts.at[self.partner()], self.partner()).start()
        for d, onward in reversed(RELAYS):
            for side in range(2):
                to = self.at(-turned(d, side), side)
                total = own(to)
                for step in onward:
                    leaf(d, step, side).wait_recv()
                    total = total + relay_in[side * per + slots[d, step]].astype(F32)
                at = side * len(relays) + relays.index(d)
                relay_out[at] = total.astype(BF16)
                final(OWN.index(d), core, relay_out.at[at], to).start()
        final(ends - 1, 1 - core, relay_out.at[0], me).wait_recv()
        sums[core] = own(me)
        sums[1 - core] = final_in[(1 - core) * ends + ends - 1].astype(F32)
        for i in reversed(range(len(OWN))):
            for half in range(2):
                final(i, half, relay_out.at[0], me).wait_recv()
                sums[half] = sums[half] + final_in[half * ends + i].astype(F32)
        whole = parts.at[pl.ds(0, 2 * (per + len(OWN)) + 1)]
        self.copy(whole, whole, send, final_sem.at[0], me).wait_send()

    def exchange(self, out, back, send, recv):
        me, ep, nz = self.me, self.ep, self.nz

        def one(to):
            self.copy(out.at[to], back.at[me], send, recv.at[me], to).start()

        def far_first(k, carry):
            offset = (nz // 2 - lax.div(k + 1, 2)) * (1 - 2 * lax.rem(k, 2))
            one(self.at(offset, 0))
            one(self.at(offset, 1))
            return carry

        lax.fori_loop(0, nz - 1, far_first, 0)
        one(self.partner())
        back[me] = out[me]

    def exchanged(self, out, back, send, recv, landed):
        me, ep = self.me, self.ep
        landed(me)

        def one(i, carry):
            frm = lax.rem(me + i, ep)
            self.copy(back.at[frm], back.at[frm], send, recv.at[frm], me).wait_recv()
            landed(frm)
            return carry

        lax.fori_loop(1, ep, one, 0)
        whole = out.at[pl.ds(0, ep - 1)]
        self.copy(whole, whole, send, recv.at[0], me).wait_send()


def tall(x, n):
    return x.reshape(n, x.shape[0] // n, x.shape[1])


def vmem():
    return pl.BlockSpec(memory_space=pltpu.VMEM)


def hbm():
    return pl.BlockSpec(memory_space=pl.ANY)


def smem():
    return pl.BlockSpec(memory_space=pltpu.SMEM)


def rows_of(dst, src, base):
    for j in range(src.shape[1] // LANES):
        dst[base + j : base + j + 1, :] = src[:, j * LANES : (j + 1) * LANES]


def row_of(dst, r, src, base, n):
    for j in range(n):
        dst[r : r + 1, j * LANES : (j + 1) * LANES] = src[base + j : base + j + 1, :]


def layer_kernel(ep, n_in, n_out, *refs):
    inputs, outputs, locals_, refs = (
        refs[:n_in], refs[n_in : n_in + n_out], refs[n_in + n_out : 2 * n_in + n_out - 1], refs[2 * n_in + n_out - 1 :]
    )
    (
        tok, mix_gain, wz, wx, wst, step_bias, decay_log, skip_gain, conv_x_w, conv_bc_w, conv_x, conv_bc, _,
        inner_gain, wo, ffn_gain, wg, wu, wd, routes, weights,
    ) = locals_
    out_ref, state, new_x, new_bc = outputs
    (
        buf, buf2, buf3, stage, narrowed, gacc, xraw, flat, out, back, tokf, convx, convbc,
        stepbc, decaybc, skipbc, bcs, ybuf, xbuf, rowx, rowbc, sq, act, wide, half_out, half_in, total,
        send_rows, relay_in, relay_out, final_in, sums,
        wload, send1, recv1, send2, recv2, send3, recv3, hsend, hrecv, xsend, xrecv, csend, relay_sem, final_sem,
    ) = refs
    comm = Comm(ep)
    me, core = comm.me, comm.core
    ready = comm.barrier()
    (
        tok_h, mix_h, wz_h, wx_h, wbc_h, wst_h, bias_h, decay_h, skip_h, cxw_h, cbw_h, cx_h, cb_h, state_h, inner_h,
        wo_h, ffn_h, wg_h, wu_h, wd_h, routes_h, weights_h,
    ) = inputs
    pairs = (
        (tok_h, tok), (cx_h, conv_x), (cxw_h, conv_x_w), (cb_h, conv_bc), (cbw_h, conv_bc_w), (routes_h, routes),
        (weights_h, weights), (skip_h, skip_gain), (bias_h, step_bias), (decay_h, decay_log), (mix_h, mix_gain),
        (inner_h, inner_gain), (ffn_h, ffn_gain),
        (wz_h, wz), (wx_h, wx), (wst_h, wst.at[pl.ds(0, 64)]), (wbc_h, wst.at[pl.ds(64, 32)]),
        (state_h, state), (wo_h, wo), (wg_h.at[0], wg), (wu_h.at[0], wu), (wd_h.at[0], wd),
    )
    pulls = [pltpu.make_async_copy(a, b, wload.at[i]) for i, (a, b) in enumerate(pairs)]
    for p in pulls:
        p.start()
    early, pulls = pulls[:13], pulls[13:]
    early[0].wait()

    rows = tok[...].astype(F32)
    for r in range(2):
        rows_of(tokf, rows[r : r + 1, :], r * 32)
    buf[me] = tall(tokf[...], 2).astype(BF16)
    ready()
    comm.gather_start(buf, send1, recv1, OWN_FIRST)
    for p in early[1:]:
        p.wait()
    for conv, taps, dst, n in ((conv_x, conv_x_w, convx, 32), (conv_bc, conv_bc_w, convbc, 8)):
        old = conv[0].astype(F32) * taps[0:1, :]
        for c in range(1, 3):
            old = old + conv[c].astype(F32) * taps[c : c + 1, :]
        for r in range(2):
            rows_of(dst, old[r : r + 1, :], r * n)
        rows_of(dst, taps[3:4, :], 2 * n)
    lane = lax.broadcasted_iota(jnp.int32, (1, LANES), 1)
    dense = jnp.zeros((1, LANES), F32)
    for r in range(2):
        for k in range(TOPK):
            dense = dense + jnp.where(lane == routes[r, k] + 32 * r, weights[r, k], 0.0)
    high = dense.astype(BF16).astype(F32)
    flat[pl.ds(3, 32, stride=8), :] = jnp.broadcast_to(high, (32, LANES))
    flat[pl.ds(7, 32, stride=8), :] = jnp.broadcast_to(dense - high, (32, LANES))
    blank = jnp.zeros((1, 64), F32)

    def column(row):
        return jnp.transpose(jnp.broadcast_to(row, (LANES, LANES)))

    skipbc[...] = column(jnp.concatenate([skip_gain[...], blank], axis=1))
    sq[...] = jnp.zeros((64, LANES), F32)

    def staged(source):
        def landed(blocks):
            for block in blocks:
                both = source[block].astype(F32)
                for r in range(2):
                    stage[pl.ds(pl.multiple_of((block * 2 + r) * PITCH, 8), 32), :] = both[r]

        return landed

    comm.gather(buf, send1, recv1, staged(buf), OWN_FIRST, RELAYS_FIRST)
    for p in pulls[:4]:
        p.wait()
    square = jnp.zeros((64, LANES), F32)
    z, x, st = jnp.zeros((64, LANES), F32), jnp.zeros((64, LANES), F32), jnp.zeros((64, 96), F32)
    for k in range(16):
        part = []
        for j in (2 * k, 2 * k + 1):
            chunk = stage[pl.ds(j, 64, stride=PITCH), :]
            square = square + chunk * chunk
            xraw[:, j * LANES : (j + 1) * LANES] = chunk.astype(BF16)
            part.append((chunk * mix_gain[j : j + 1, :]).astype(BF16))
        part = jnp.concatenate(part, axis=1)
        at = slice(k * 256, (k + 1) * 256)
        z = z + jnp.dot(part, wz[at, :], preferred_element_type=F32)
        x = x + jnp.dot(part, wx[at, :], preferred_element_type=F32)
        st = st + lax.dot_general(part, wst[:, at], (((1,), (1,)), ((), ())), preferred_element_type=F32)
    scale = lax.rsqrt(jnp.sum(square, axis=1, keepdims=True) / 4096.0 + 1e-6)
    z, x, st = z * scale, x * scale, st * scale
    flat[pl.ds(0, 64, stride=4), :] = z
    flat[pl.ds(1, 64, stride=4), :] = x
    bc = st[:, 64:96]
    spread = jnp.concatenate([bc, bc, bc, bc], axis=1)
    flat[pl.ds(2, 64, stride=4), :] = jnp.where(lax.div(lane, 32) == lax.rem(me, 4), spread, 0.0)
    out[...] = tall(flat[...], 32).astype(BF16)
    comm.exchange(out, back, xsend, xrecv)

    flat[pl.ds(0, 64, stride=4), :] = jnp.concatenate([st[:, 0:64], st[:, 0:64]], axis=1)
    mine8 = flat[pl.ds(pl.multiple_of(me * 8, 8), 8), :]
    bias = jnp.concatenate([step_bias[...], blank], axis=1)
    rate = jnp.exp(jnp.concatenate([decay_log[...], blank], axis=1))
    for r in range(2):
        step = jax.nn.softplus(mine8[r * 4 : r * 4 + 1, :] + bias)
        stepbc[pl.ds(r * LANES, LANES), :] = column(step)
        decaybc[pl.ds(r * LANES, LANES), :] = column(jnp.exp(-step * rate))
    low = lax.broadcasted_iota(jnp.int32, (32, LANES), 1) < 64

    def spread_heads(source, base):
        return jnp.where(
            low, source[pl.ds(base, 32, stride=2), :], source[pl.ds(base + 1, 32, stride=2), :]
        )

    gacc[...] = jnp.zeros((64, 1024), F32)
    pulls[4].wait()

    def narrow(i, carry):
        r, g = lax.div(i, 4), lax.rem(i, 4)
        heads = state[r, pl.ds(g * 16, 16)].reshape(1024, LANES)
        narrowed[pl.ds(pl.multiple_of(i * 1024, 1024), 1024), :] = heads.astype(BF16)
        return carry

    lax.fori_loop(0, 8, narrow, 0)
    comm.exchanged(out, back, xsend, xrecv, lambda frm: None)
    flat[...] = back[...].astype(F32).reshape(256, LANES)
    for r in range(2):
        x_pre = flat[pl.ds(4 * r + 1, 32, stride=8), :]
        bc_pre = flat[pl.ds(4 * r + 2, 8, stride=32), :]
        for q in range(1, 4):
            bc_pre = bc_pre + flat[pl.ds(8 * q + 4 * r + 2, 8, stride=32), :]
        xbuf[pl.ds(r * 32, 32), :] = x_pre
        bcs[pl.ds(16 + r * 8, 8), :] = bc_pre
        xc = jax.nn.silu(convx[pl.ds(r * 32, 32), :] + convx[pl.ds(64, 32), :] * x_pre)
        maps = jax.nn.silu(convbc[pl.ds(r * 8, 8), :] + convbc[pl.ds(16, 8), :] * bc_pre)
        bcs[pl.ds(r * 8, 8), :] = maps
        fed = spread_heads(stepbc, r * LANES) * xc
        total[pl.ds(r * 32, 32), :] = fed
        both = jnp.sum(maps[0:4, :] * maps[4:8, :], axis=1, keepdims=True)
        for g in range(4):
            i = r * 4 + g
            y = lax.dot_general(
                jnp.broadcast_to(maps[4 + g : 5 + g, :], (8, LANES)).astype(BF16),
                narrowed[i * 1024 : (i + 1) * 1024, :],
                (((1,), (1,)), ((), ())),
                preferred_element_type=F32,
            )
            for k in range(8):
                ybuf[i * 8 + k : i * 8 + k + 1, :] = y[0:1, k * LANES : (k + 1) * LANES]
        boths = jnp.concatenate([jnp.broadcast_to(both[g : g + 1, :], (8, LANES)) for g in range(4)], axis=0)
        gated = spread_heads(decaybc, r * LANES) * ybuf[pl.ds(r * 32, 32), :] + fed * boths
        gated = gated + spread_heads(skipbc, 0) * xc
        gated = gated * jax.nn.silu(flat[pl.ds(4 * r, 32, stride=8), :])
        mean = jnp.sum(jnp.sum(gated * gated, axis=1, keepdims=True), axis=0, keepdims=True) / 4096.0
        buf2[me, r] = (gated * lax.rsqrt(mean + 1e-6) * inner_gain[...]).astype(BF16)

    def group(i, carry):
        r, g = lax.div(i, 4), lax.rem(i, 4)
        cols = jnp.transpose(total[pl.ds(pl.multiple_of(i * 8, 8), 8), :])
        into = jnp.broadcast_to(bcs[pl.ds(r * 8 + g, 1), :], (LANES, LANES))
        for k in range(8):
            h = g * 16 + 2 * k
            dec = jnp.concatenate(
                [
                    jnp.broadcast_to(decaybc[pl.ds(r * LANES + h, 1), :], (64, LANES)),
                    jnp.broadcast_to(decaybc[pl.ds(r * LANES + h + 1, 1), :], (64, LANES)),
                ],
                axis=0,
            )
            new = dec * state[r, pl.ds(h, 2)].reshape(LANES, LANES)
            new = new + jnp.broadcast_to(cols[:, k : k + 1], (LANES, LANES)) * into
            state[r, pl.ds(h, 2)] = new.reshape(2, 64, LANES)
        return carry

    comm.gather_start(buf2, send2, recv2)
    for r in range(2):
        row_of(rowx, r, xbuf, r * 32, 32)
        row_of(rowbc, r, bcs, 16 + r * 8, 8)
    for old, new, row in ((conv_x, new_x, rowx), (conv_bc, new_bc, rowbc)):
        new[0] = old[1]
        new[1] = old[2]
        new[2] = row[...].astype(BF16)
    lax.fori_loop(0, 4, group, 0)
    comm.gather(buf2, send2, recv2, staged(buf2))
    pulls[5].wait()
    cols_out = jnp.zeros((64, LANES), F32)
    for k in range(16):
        part = [stage[pl.ds(j, 64, stride=PITCH), :].astype(BF16) for j in (2 * k, 2 * k + 1)]
        part = jnp.concatenate(part, axis=1)
        cols_out = cols_out + jnp.dot(part, wo[k * 256 : (k + 1) * 256, :], preferred_element_type=F32)
    buf3[me] = cols_out.astype(BF16)

    def landed3(blocks):
        gates, ups, square = gacc[:, 0:512], gacc[:, 512:1024], sq[...]
        for pair in zip(blocks[::2], blocks[1::2], strict=True):
            part, gate_rows, up_rows = [], [], []
            for block in pair:
                cols = pl.ds(pl.multiple_of(block * LANES, LANES), LANES)
                resid = (xraw[:, cols].astype(F32) + buf3[block].astype(F32)).astype(BF16).astype(F32)
                square = square + resid * resid
                stage[pl.ds(block, 64, stride=PITCH), :] = resid
                part.append((resid * ffn_gain[pl.ds(block, 1), :]).astype(BF16))
                gate_rows.append(wg[cols, :])
                up_rows.append(wu[cols, :])
            part = jnp.concatenate(part, axis=1)
            gates = gates + jnp.dot(part, jnp.concatenate(gate_rows, axis=0), preferred_element_type=F32)
            ups = ups + jnp.dot(part, jnp.concatenate(up_rows, axis=0), preferred_element_type=F32)
        gacc[:, 0:512], gacc[:, 512:1024], sq[...] = gates, ups, square

    comm.gather_start(buf3, send3, recv3)
    lax.fori_loop(4, 8, group, 0)
    pulls[6].wait()
    pulls[7].wait()
    comm.gather(buf3, send3, recv3, landed3)
    scale = lax.rsqrt(jnp.sum(sq[...], axis=1, keepdims=True) / 4096.0 + 1e-6)
    gate, up = gacc[:, 0:512] * scale, gacc[:, 512:1024] * scale
    act[...] = (jax.nn.silu(gate) * up).astype(BF16)
    pulls[8].wait()
    lanes32 = lax.broadcasted_iota(jnp.int32, (32, LANES), 1)
    dense = flat[pl.ds(3, 32, stride=8), :] + flat[pl.ds(7, 32, stride=8), :]
    for r in range(2):
        picked = jnp.sum(jnp.where(lanes32 == me + 32 * r, dense, 0.0), axis=1, keepdims=True)
        wide[pl.ds(r, 32, stride=2), :] = jnp.broadcast_to(picked, (32, LANES))
    weight = jnp.concatenate([wide[...]] * 4, axis=1)

    def expert(half, part):
        at = pl.ds(pl.multiple_of(half * 2048 + part * 512, 512), 512)
        y = jnp.dot(act[...], wd[:, at], preferred_element_type=F32).astype(BF16).astype(F32)
        return y * weight

    swaps = []
    for ch in range(2):
        for k in range(2):
            half_out[ch, :, k * 512 : (k + 1) * 512] = expert(1 - core, 2 * ch + k).astype(BF16)
        swaps.append(
            comm.copy(half_out.at[ch], half_in.at[ch], hsend.at[ch], hrecv.at[ch], comm.partner())
        )
        swaps[ch].start()
    for ch in range(2):
        own = [expert(core, 2 * ch + k) for k in range(2)]
        swaps[ch].wait()
        for j in range(8):
            k, cols = j // 4, slice(j % 4 * LANES, (j % 4 + 1) * LANES)
            total[pl.ds(8 * ch + j, 64, stride=24), :] = own[k][:, cols] + half_in[
                ch, :, j * LANES : (j + 1) * LANES
            ].astype(F32)


    def pack(t, carry):
        for r in range(2):
            send_rows[t, r] = total[pl.ds(pl.multiple_of((t * 2 + r) * 24, 8), 16), :].astype(BF16)
        return carry

    lax.fori_loop(0, ep, pack, 0)

    def chip_rows(device):
        at = [pl.ds(pl.multiple_of((device * 2 + r) * 24, 8), 16) for r in range(2)]
        return jnp.stack([total[a, :] for a in at])

    for r in range(2):
        tokf[pl.ds(r * 32, 32), :] = stage[pl.ds(pl.multiple_of((me * 2 + r) * PITCH, 8), 32), :]
    comm.reduce(chip_rows, send_rows, relay_in, relay_out, final_in, sums, csend, relay_sem, final_sem)
    for half in range(2):
        for r in range(2):
            at = pl.ds(r * 32 + half * 16, 16)
            tokf[at, :] = tokf[at, :] + sums[half, r]
    for r in range(2):
        row_of(rowx, r, tokf, r * 32, 32)
    out_ref[...] = rowx[...].astype(BF16)


def layer(ep, *args):
    dma = pltpu.SemaphoreType.DMA
    v = pltpu.VMEM
    local = [v(a.shape[1:] if a.shape[0] == 1 and a.ndim == 3 else a.shape, a.dtype) for a in args]
    local[4:6] = [v((96, 4096), BF16)]
    del local[12]
    local.insert(12, v((8, LANES), F32))
    local[-2:] = [pltpu.SMEM(a.shape, a.dtype) for a in args[-2:]]
    outs = (
        jax.ShapeDtypeStruct((2, 4096), BF16),
        jax.ShapeDtypeStruct(args[13].shape, F32),
        jax.ShapeDtypeStruct(args[11].shape, BF16),
        jax.ShapeDtypeStruct(args[12].shape, BF16),
    )
    results = pl.pallas_call(
        functools.partial(layer_kernel, ep, len(args), len(outs)),
        out_shape=outs,
        in_specs=[hbm()] * len(args),
        out_specs=(vmem(),) * len(outs),
        scratch_shapes=[
            *local,
            v((ep, 2, 32, LANES), BF16), v((ep, 2, 32, LANES), BF16), v((ep, 64, LANES), BF16),
            v((64 * PITCH, LANES), F32), v((8192, LANES), BF16), v((64, 1024), F32), v((64, 4096), BF16),
            v((256, LANES), F32), v((ep, 8, LANES), BF16), v((ep, 8, LANES), BF16), v((64, LANES), F32),
            v((96, LANES), F32), v((24, LANES), F32),
            v((256, LANES), F32), v((256, LANES), F32), v((LANES, LANES), F32), v((32, LANES), F32),
            v((64, LANES), F32), v((64, LANES), F32), v((2, 4096), F32), v((2, 1024), F32), v((64, LANES), F32),
            v((64, 512), BF16), v((64, LANES), F32), v((2, 64, 1024), BF16), v((2, 64, 1024), BF16),
            v((64 * 24, LANES), F32),
            v((ep, 2, 16, LANES), BF16), v((18, 2, 16, LANES), BF16), v((8, 2, 16, LANES), BF16),
            v((14, 2, 16, LANES), BF16), v((2, 2, 16, LANES), F32),
            dma((22,)), dma, dma((ep,)), dma, dma((ep,)), dma, dma((ep,)), dma((2,)), dma((2,)), dma, dma((ep,)),
            dma, dma((18,)), dma((14,)),
        ],
        compiler_params=pltpu.CompilerParams(
            collective_id=0, has_side_effects=True, vmem_limit_bytes=VMEM_LIMIT
        ),
        name="layer",
    )(*(pltpu.with_memory_space_constraint(a, pltpu.HBM) for a in args))
    return pl.pallas_call(
        flush_kernel,
        out_shape=outs,
        in_specs=[vmem()] * len(outs),
        out_specs=(hbm(),) * len(outs),
        scratch_shapes=[dma((len(outs),))],
        compiler_params=pltpu.CompilerParams(vmem_limit_bytes=1024 * 1024),
        name="flush",
    )(*results)


def flush_kernel(*refs):
    n = len(refs) // 2
    copies = [pltpu.make_async_copy(refs[i], refs[n + i], refs[-1].at[i]) for i in range(n)]
    for c in copies:
        c.start()
    for c in copies:
        c.wait()


def body(
    ep, tokens_in, mix_gain, w_gate_z, w_value, w_in_bc, w_step, step_bias, decay_log, skip_gain, conv_x_weight,
    conv_bc_weight, conv_x_state, conv_bc_state, ssm_state, inner_gain, out_weight, ffn_gain, expert_gate,
    expert_up, expert_down, routes, route_weight,
):
    out, new_state, new_x, new_bc = layer(
        ep, tokens_in, mix_gain.reshape(32, LANES), w_gate_z, w_value, w_in_bc.T, w_step.T,
        step_bias.reshape(1, 64), decay_log.reshape(1, 64), skip_gain.reshape(1, 64), conv_x_weight,
        conv_bc_weight, conv_x_state.transpose(1, 0, 2), conv_bc_state.transpose(1, 0, 2), ssm_state,
        inner_gain.reshape(32, LANES), out_weight, ffn_gain.reshape(32, LANES), expert_gate, expert_up,
        expert_down, routes, route_weight,
    )
    return out, new_state, new_x.transpose(1, 0, 2), new_bc.transpose(1, 0, 2)


def solution(mesh):
    ep = mesh.shape["ep"]
    cols, rep = P(None, "ep"), P()
    placed = (
        P(GRP_EP, None), rep, cols, cols, cols, rep, rep, rep, rep, rep, rep,
        P(GRP_EP, None, None), P(GRP_EP, None, None), P(GRP_EP, None, None, None),
        rep, cols, rep, P("ep", None, None), P("ep", None, None), P("ep", None, None),
        P(GRP_EP, None), P(GRP_EP, None),
    )
    return jax.shard_map(
        functools.partial(body, ep),
        mesh=mesh,
        in_specs=placed,
        out_specs=(
            P(GRP_EP, None),
            P(GRP_EP, None, None, None),
            P(GRP_EP, None, None),
            P(GRP_EP, None, None),
        ),
        check_vma=False,
    )
```

```python
import functools

import jax
import jax.numpy as jnp
from jax import lax
from jax.experimental import pallas as pl
from jax.experimental.pallas import tpu as pltpu
from jax.sharding import PartitionSpec as P

TOPK = 4
GRP_EP = ("grp", "ep")
MESH = pl.DeviceIdType.MESH
F32 = jnp.float32
BF16 = jnp.bfloat16
LANES = 128
PITCH = 40
VMEM_LIMIT = 38 * 1024 * 1024

OWN = (6, -6, 3, -3, 1, -1)
RELAYS = ((3, (1, -1)), (-3, (1, -1)), (6, (2, 1, -1)), (-6, (1, -1)))
OWN_FIRST = (3, -3, 1, -1)
RELAYS_FIRST = ((3, (3, 1, -1)), (-3, (-3, 1, -1)), (6, (2, 1, -1)), (-6, (1, -1)))
GREET = (1, -1, 2, -2, 3, -3)
GROUPS = ((1, -1), (3, -3), (6, -6, 2, -2, 4, -4), (5, -5, 7, -7), (8,))


def turned(d, side):
    return d if side == 0 else -d


class Comm:
    def __init__(self, ep):
        self.ep = ep
        self.nz = ep // 2
        self.me = lax.axis_index("ep")
        self.core = lax.rem(self.me, 2)
        self.z = lax.div(self.me, 2)

    def at(self, offset, core):
        return lax.rem(self.z + offset + self.nz, self.nz) * 2 + core

    def partner(self):
        return self.z * 2 + (1 - self.core)

    def barrier(self):
        sem = pltpu.get_barrier_semaphore()

        def greet(to):
            pl.semaphore_signal(sem, inc=1, device_id={"ep": to}, device_id_type=MESH)

        @pl.when(self.core == 1)
        def _():
            for d in GREET:
                greet(self.at(d, 0))
                greet(self.at(d, 1))

        greet(self.partner())
        return lambda: pl.semaphore_wait(sem, len(GREET) + 1)

    def copy(self, src, dst, send, recv, to):
        return pltpu.make_async_remote_copy(
            src_ref=src, dst_ref=dst, send_sem=send, recv_sem=recv, device_id={"ep": to}, device_id_type=MESH
        )

    def gather_start(self, buf, send, recv, own=OWN):
        me = self.me
        for to in [self.at(d * (1 - 2 * self.core), 1) for d in own] + [self.partner()]:
            self.copy(buf.at[me], buf.at[me], send, recv.at[me], to).start()

    def gather(self, buf, send, recv, landed, own=OWN, onward=RELAYS):
        core, me = self.core, self.me

        def pass_on(block, to):
            self.copy(buf.at[block], buf.at[block], send, recv.at[block], to).start()

        def arrive(block):
            self.copy(buf.at[block], buf.at[block], send, recv.at[block], me).wait_recv()

        def sent(n):
            whole = buf.at[pl.ds(0, n)]
            self.copy(whole, whole, send, recv.at[0], me).wait_send()

        relays = dict(onward)

        @pl.when(core == 1)
        def _():
            arrive(self.partner())
            blocks, passed = [me, self.partner()], 0
            for offsets in GROUPS:
                for d in offsets:
                    for side in range(2):
                        block = self.at(-turned(d, side), side)
                        arrive(block)
                        for step in relays.get(d, ()):
                            pass_on(block, self.at(turned(step, side), 1))
                            passed += 1
                        pass_on(block, self.partner())
                        passed += 1
                        blocks.append(block)
                if offsets == GROUPS[-2]:
                    continue
                landed(blocks)
                blocks = []
            sent(len(own) + 1)
            for start in range(0, passed, self.ep):
                sent(min(self.ep, passed - start))

        @pl.when(core == 0)
        def _():
            arrive(self.partner())
            blocks = [me, self.partner()]
            for offsets in GROUPS:
                for d in offsets:
                    for side in range(2):
                        block = self.at(-turned(d, side), side)
                        arrive(block)
                        blocks.append(block)
                landed(blocks)
                blocks = []
            sent(len(own) + 1)

    def reduce(self, own, parts, relay_in, relay_out, final_in, sums, send, relay_sem, final_sem):
        core, me = self.core, self.me
        slots = {(d, step): i for i, (d, step) in enumerate((d, step) for d, on in RELAYS for step in on)}
        relays = [d for d, _ in RELAYS]
        per, ends = len(slots), len(OWN) + 1

        def leaf(d, step, side):
            slot = side * per + slots[d, step]
            to = self.at(-turned(step, side), core)
            part = parts.at[self.at(-turned(d + step, side), side)]
            return self.copy(part, relay_in.at[slot], send, relay_sem.at[slot], to)

        def final(i, half, source, to):
            slot = half * ends + i
            return self.copy(source, final_in.at[slot], send, final_sem.at[slot], to)

        for d, onward in reversed(RELAYS):
            for step in onward:
                for side in range(2):
                    leaf(d, step, side).start()
        for i, d in enumerate(OWN):
            if d not in relays:
                for side in range(2):
                    to = self.at(-turned(d, side), side)
                    final(i, core, parts.at[to], to).start()
        final(ends - 1, core, parts.at[self.partner()], self.partner()).start()
        for d, onward in reversed(RELAYS):
            for side in range(2):
                to = self.at(-turned(d, side), side)
                total = own(to)
                for step in onward:
                    leaf(d, step, side).wait_recv()
                    total = total + relay_in[side * per + slots[d, step]].astype(F32)
                at = side * len(relays) + relays.index(d)
                relay_out[at] = total.astype(BF16)
                final(OWN.index(d), core, relay_out.at[at], to).start()
        final(ends - 1, 1 - core, relay_out.at[0], me).wait_recv()
        sums[core] = own(me)
        sums[1 - core] = final_in[(1 - core) * ends + ends - 1].astype(F32)
        for i in reversed(range(len(OWN))):
            for half in range(2):
                final(i, half, relay_out.at[0], me).wait_recv()
                sums[half] = sums[half] + final_in[half * ends + i].astype(F32)
        whole = parts.at[pl.ds(0, 2 * (per + len(OWN)) + 1)]
        self.copy(whole, whole, send, final_sem.at[0], me).wait_send()

    def exchange(self, out, back, send, recv):
        me, ep, nz = self.me, self.ep, self.nz

        def one(to):
            self.copy(out.at[to], back.at[me], send, recv.at[me], to).start()

        def far_first(k, carry):
            offset = (nz // 2 - lax.div(k + 1, 2)) * (1 - 2 * lax.rem(k, 2))
            one(self.at(offset, 0))
            one(self.at(offset, 1))
            return carry

        lax.fori_loop(0, nz - 1, far_first, 0)
        one(self.partner())
        back[me] = out[me]

    def exchanged(self, out, back, send, recv, landed):
        me, ep = self.me, self.ep
        landed(me)

        def one(i, carry):
            frm = lax.rem(me + i, ep)
            self.copy(back.at[frm], back.at[frm], send, recv.at[frm], me).wait_recv()
            landed(frm)
            return carry

        lax.fori_loop(1, ep, one, 0)
        whole = out.at[pl.ds(0, ep - 1)]
        self.copy(whole, whole, send, recv.at[0], me).wait_send()


def tall(x, n):
    return x.reshape(n, x.shape[0] // n, x.shape[1])


def vmem():
    return pl.BlockSpec(memory_space=pltpu.VMEM)


def hbm():
    return pl.BlockSpec(memory_space=pl.ANY)


def smem():
    return pl.BlockSpec(memory_space=pltpu.SMEM)


def rows_of(dst, src, base):
    for j in range(src.shape[1] // LANES):
        dst[base + j : base + j + 1, :] = src[:, j * LANES : (j + 1) * LANES]


def row_of(dst, r, src, base, n):
    for j in range(n):
        dst[r : r + 1, j * LANES : (j + 1) * LANES] = src[base + j : base + j + 1, :]


def layer_kernel(ep, n_in, n_out, *refs):
    inputs, outputs, locals_, refs = (
        refs[:n_in], refs[n_in : n_in + n_out], refs[n_in + n_out : 2 * n_in + n_out - 1], refs[2 * n_in + n_out - 1 :]
    )
    (
        tok, mix_gain, wz, wx, wst, step_bias, decay_log, skip_gain, conv_x_w, conv_bc_w, conv_x, conv_bc, _,
        inner_gain, wo, ffn_gain, wg, wu, wd, routes, weights,
    ) = locals_
    out_ref, state, new_x, new_bc = outputs
    (
        buf, buf2, buf3, stage, narrowed, gacc, xraw, flat, out, back, tokf, convx, convbc,
        stepbc, decaybc, skipbc, bcs, ybuf, xbuf, rowx, rowbc, sq, act, wide, half_out, half_in, total,
        send_rows, relay_in, relay_out, final_in, sums,
        wload, send1, recv1, send2, recv2, send3, recv3, hsend, hrecv, xsend, xrecv, csend, relay_sem, final_sem,
    ) = refs
    comm = Comm(ep)
    me, core = comm.me, comm.core
    ready = comm.barrier()
    (
        tok_h, mix_h, wz_h, wx_h, wbc_h, wst_h, bias_h, decay_h, skip_h, cxw_h, cbw_h, cx_h, cb_h, state_h, inner_h,
        wo_h, ffn_h, wg_h, wu_h, wd_h, routes_h, weights_h,
    ) = inputs
    pairs = (
        (tok_h, tok), (cx_h, conv_x), (cxw_h, conv_x_w), (cb_h, conv_bc), (cbw_h, conv_bc_w), (routes_h, routes),
        (weights_h, weights), (skip_h, skip_gain), (bias_h, step_bias), (decay_h, decay_log), (mix_h, mix_gain),
        (inner_h, inner_gain), (ffn_h, ffn_gain),
        (wz_h, wz), (wx_h, wx), (wst_h, wst.at[pl.ds(0, 64)]), (wbc_h, wst.at[pl.ds(64, 32)]),
        (state_h, state), (wo_h, wo), (wg_h.at[0], wg), (wu_h.at[0], wu), (wd_h.at[0], wd),
    )
    pulls = [pltpu.make_async_copy(a, b, wload.at[i]) for i, (a, b) in enumerate(pairs)]
    pulls[0].start()
    pulls[0].wait()

    rows = tok[...].astype(F32)
    for r in range(2):
        rows_of(tokf, rows[r : r + 1, :], r * 32)
    buf[me] = tall(tokf[...], 2).astype(BF16)
    ready()
    comm.gather_start(buf, send1, recv1, OWN_FIRST)
    for p in pulls[1:]:
        p.start()
    early, pulls = pulls[:13], pulls[13:]
    for p in early[1:]:
        p.wait()
    for conv, taps, dst, n in ((conv_x, conv_x_w, convx, 32), (conv_bc, conv_bc_w, convbc, 8)):
        old = conv[0].astype(F32) * taps[0:1, :]
        for c in range(1, 3):
            old = old + conv[c].astype(F32) * taps[c : c + 1, :]
        for r in range(2):
            rows_of(dst, old[r : r + 1, :], r * n)
        rows_of(dst, taps[3:4, :], 2 * n)
    lane = lax.broadcasted_iota(jnp.int32, (1, LANES), 1)
    dense = jnp.zeros((1, LANES), F32)
    for r in range(2):
        for k in range(TOPK):
            dense = dense + jnp.where(lane == routes[r, k] + 32 * r, weights[r, k], 0.0)
    high = dense.astype(BF16).astype(F32)
    flat[pl.ds(3, 32, stride=8), :] = jnp.broadcast_to(high, (32, LANES))
    flat[pl.ds(7, 32, stride=8), :] = jnp.broadcast_to(dense - high, (32, LANES))
    blank = jnp.zeros((1, 64), F32)

    def column(row):
        return jnp.transpose(jnp.broadcast_to(row, (LANES, LANES)))

    skipbc[...] = column(jnp.concatenate([skip_gain[...], blank], axis=1))
    sq[...] = jnp.zeros((64, LANES), F32)

    def staged(source):
        def landed(blocks):
            for block in blocks:
                both = source[block].astype(F32)
                for r in range(2):
                    stage[pl.ds(pl.multiple_of((block * 2 + r) * PITCH, 8), 32), :] = both[r]

        return landed

    comm.gather(buf, send1, recv1, staged(buf), OWN_FIRST, RELAYS_FIRST)
    for p in pulls[:4]:
        p.wait()
    square = jnp.zeros((64, LANES), F32)
    z, x, st = jnp.zeros((64, LANES), F32), jnp.zeros((64, LANES), F32), jnp.zeros((64, 96), F32)
    for k in range(16):
        part = []
        for j in (2 * k, 2 * k + 1):
            chunk = stage[pl.ds(j, 64, stride=PITCH), :]
            square = square + chunk * chunk
            xraw[:, j * LANES : (j + 1) * LANES] = chunk.astype(BF16)
            part.append((chunk * mix_gain[j : j + 1, :]).astype(BF16))
        part = jnp.concatenate(part, axis=1)
        at = slice(k * 256, (k + 1) * 256)
        z = z + jnp.dot(part, wz[at, :], preferred_element_type=F32)
        x = x + jnp.dot(part, wx[at, :], preferred_element_type=F32)
        st = st + lax.dot_general(part, wst[:, at], (((1,), (1,)), ((), ())), preferred_element_type=F32)
    scale = lax.rsqrt(jnp.sum(square, axis=1, keepdims=True) / 4096.0 + 1e-6)
    z, x, st = z * scale, x * scale, st * scale
    flat[pl.ds(0, 64, stride=4), :] = z
    flat[pl.ds(1, 64, stride=4), :] = x
    bc = st[:, 64:96]
    spread = jnp.concatenate([bc, bc, bc, bc], axis=1)
    flat[pl.ds(2, 64, stride=4), :] = jnp.where(lax.div(lane, 32) == lax.rem(me, 4), spread, 0.0)
    out[...] = tall(flat[...], 32).astype(BF16)
    comm.exchange(out, back, xsend, xrecv)

    flat[pl.ds(0, 64, stride=4), :] = jnp.concatenate([st[:, 0:64], st[:, 0:64]], axis=1)
    mine8 = flat[pl.ds(pl.multiple_of(me * 8, 8), 8), :]
    bias = jnp.concatenate([step_bias[...], blank], axis=1)
    rate = jnp.exp(jnp.concatenate([decay_log[...], blank], axis=1))
    for r in range(2):
        step = jax.nn.softplus(mine8[r * 4 : r * 4 + 1, :] + bias)
        stepbc[pl.ds(r * LANES, LANES), :] = column(step)
        decaybc[pl.ds(r * LANES, LANES), :] = column(jnp.exp(-step * rate))
    low = lax.broadcasted_iota(jnp.int32, (32, LANES), 1) < 64

    def spread_heads(source, base):
        return jnp.where(
            low, source[pl.ds(base, 32, stride=2), :], source[pl.ds(base + 1, 32, stride=2), :]
        )

    gacc[...] = jnp.zeros((64, 1024), F32)
    pulls[4].wait()

    def narrow(i, carry):
        r, g = lax.div(i, 4), lax.rem(i, 4)
        heads = state[r, pl.ds(g * 16, 16)].reshape(1024, LANES)
        narrowed[pl.ds(pl.multiple_of(i * 1024, 1024), 1024), :] = heads.astype(BF16)
        return carry

    lax.fori_loop(0, 8, narrow, 0)
    comm.exchanged(out, back, xsend, xrecv, lambda frm: None)
    flat[...] = back[...].astype(F32).reshape(256, LANES)
    for r in range(2):
        x_pre = flat[pl.ds(4 * r + 1, 32, stride=8), :]
        bc_pre = flat[pl.ds(4 * r + 2, 8, stride=32), :]
        for q in range(1, 4):
            bc_pre = bc_pre + flat[pl.ds(8 * q + 4 * r + 2, 8, stride=32), :]
        xbuf[pl.ds(r * 32, 32), :] = x_pre
        bcs[pl.ds(16 + r * 8, 8), :] = bc_pre
        xc = jax.nn.silu(convx[pl.ds(r * 32, 32), :] + convx[pl.ds(64, 32), :] * x_pre)
        maps = jax.nn.silu(convbc[pl.ds(r * 8, 8), :] + convbc[pl.ds(16, 8), :] * bc_pre)
        bcs[pl.ds(r * 8, 8), :] = maps
        fed = spread_heads(stepbc, r * LANES) * xc
        total[pl.ds(r * 32, 32), :] = fed
        both = jnp.sum(maps[0:4, :] * maps[4:8, :], axis=1, keepdims=True)
        for g in range(4):
            i = r * 4 + g
            y = lax.dot_general(
                jnp.broadcast_to(maps[4 + g : 5 + g, :], (8, LANES)).astype(BF16),
                narrowed[i * 1024 : (i + 1) * 1024, :],
                (((1,), (1,)), ((), ())),
                preferred_element_type=F32,
            )
            for k in range(8):
                ybuf[i * 8 + k : i * 8 + k + 1, :] = y[0:1, k * LANES : (k + 1) * LANES]
        boths = jnp.concatenate([jnp.broadcast_to(both[g : g + 1, :], (8, LANES)) for g in range(4)], axis=0)
        gated = spread_heads(decaybc, r * LANES) * ybuf[pl.ds(r * 32, 32), :] + fed * boths
        gated = gated + spread_heads(skipbc, 0) * xc
        gated = gated * jax.nn.silu(flat[pl.ds(4 * r, 32, stride=8), :])
        mean = jnp.sum(jnp.sum(gated * gated, axis=1, keepdims=True), axis=0, keepdims=True) / 4096.0
        buf2[me, r] = (gated * lax.rsqrt(mean + 1e-6) * inner_gain[...]).astype(BF16)

    def group(i, carry):
        r, g = lax.div(i, 4), lax.rem(i, 4)
        cols = jnp.transpose(total[pl.ds(pl.multiple_of(i * 8, 8), 8), :])
        into = jnp.broadcast_to(bcs[pl.ds(r * 8 + g, 1), :], (LANES, LANES))
        for k in range(8):
            h = g * 16 + 2 * k
            dec = jnp.concatenate(
                [
                    jnp.broadcast_to(decaybc[pl.ds(r * LANES + h, 1), :], (64, LANES)),
                    jnp.broadcast_to(decaybc[pl.ds(r * LANES + h + 1, 1), :], (64, LANES)),
                ],
                axis=0,
            )
            new = dec * state[r, pl.ds(h, 2)].reshape(LANES, LANES)
            new = new + jnp.broadcast_to(cols[:, k : k + 1], (LANES, LANES)) * into
            state[r, pl.ds(h, 2)] = new.reshape(2, 64, LANES)
        return carry

    comm.gather_start(buf2, send2, recv2)
    for r in range(2):
        row_of(rowx, r, xbuf, r * 32, 32)
        row_of(rowbc, r, bcs, 16 + r * 8, 8)
    for old, new, row in ((conv_x, new_x, rowx), (conv_bc, new_bc, rowbc)):
        new[0] = old[1]
        new[1] = old[2]
        new[2] = row[...].astype(BF16)
    lax.fori_loop(0, 4, group, 0)
    comm.gather(buf2, send2, recv2, staged(buf2))
    pulls[5].wait()
    cols_out = jnp.zeros((64, LANES), F32)
    for k in range(16):
        part = [stage[pl.ds(j, 64, stride=PITCH), :].astype(BF16) for j in (2 * k, 2 * k + 1)]
        part = jnp.concatenate(part, axis=1)
        cols_out = cols_out + jnp.dot(part, wo[k * 256 : (k + 1) * 256, :], preferred_element_type=F32)
    buf3[me] = cols_out.astype(BF16)

    def landed3(blocks):
        gates, ups, square = gacc[:, 0:512], gacc[:, 512:1024], sq[...]
        for pair in zip(blocks[::2], blocks[1::2], strict=True):
            part, gate_rows, up_rows = [], [], []
            for block in pair:
                cols = pl.ds(pl.multiple_of(block * LANES, LANES), LANES)
                resid = (xraw[:, cols].astype(F32) + buf3[block].astype(F32)).astype(BF16).astype(F32)
                square = square + resid * resid
                stage[pl.ds(block, 64, stride=PITCH), :] = resid
                part.append((resid * ffn_gain[pl.ds(block, 1), :]).astype(BF16))
                gate_rows.append(wg[cols, :])
                up_rows.append(wu[cols, :])
            part = jnp.concatenate(part, axis=1)
            gates = gates + jnp.dot(part, jnp.concatenate(gate_rows, axis=0), preferred_element_type=F32)
            ups = ups + jnp.dot(part, jnp.concatenate(up_rows, axis=0), preferred_element_type=F32)
        gacc[:, 0:512], gacc[:, 512:1024], sq[...] = gates, ups, square

    comm.gather_start(buf3, send3, recv3)
    lax.fori_loop(4, 8, group, 0)
    pulls[6].wait()
    pulls[7].wait()
    comm.gather(buf3, send3, recv3, landed3)
    scale = lax.rsqrt(jnp.sum(sq[...], axis=1, keepdims=True) / 4096.0 + 1e-6)
    gate, up = gacc[:, 0:512] * scale, gacc[:, 512:1024] * scale
    act[...] = (jax.nn.silu(gate) * up).astype(BF16)
    pulls[8].wait()
    lanes32 = lax.broadcasted_iota(jnp.int32, (32, LANES), 1)
    dense = flat[pl.ds(3, 32, stride=8), :] + flat[pl.ds(7, 32, stride=8), :]
    for r in range(2):
        picked = jnp.sum(jnp.where(lanes32 == me + 32 * r, dense, 0.0), axis=1, keepdims=True)
        wide[pl.ds(r, 32, stride=2), :] = jnp.broadcast_to(picked, (32, LANES))
    weight = jnp.concatenate([wide[...]] * 4, axis=1)

    def expert(half, part):
        at = pl.ds(pl.multiple_of(half * 2048 + part * 512, 512), 512)
        y = jnp.dot(act[...], wd[:, at], preferred_element_type=F32).astype(BF16).astype(F32)
        return y * weight

    swaps = []
    for k in range(4):
        half_out[k] = expert(1 - core, k).astype(BF16)
        swaps.append(comm.copy(half_out.at[k], half_in.at[k], hsend.at[k], hrecv.at[k], comm.partner()))
        swaps[k].start()
    for k in range(4):
        own = expert(core, k)
        swaps[k].wait()
        own = own + half_in[k].astype(F32)
        for j in range(4):
            total[pl.ds(4 * k + j, 64, stride=24), :] = own[:, j * LANES : (j + 1) * LANES]

    def pack(t, carry):
        for r in range(2):
            send_rows[t, r] = total[pl.ds(pl.multiple_of((t * 2 + r) * 24, 8), 16), :].astype(BF16)
        return carry

    lax.fori_loop(0, ep, pack, 0)

    def chip_rows(device):
        at = [pl.ds(pl.multiple_of((device * 2 + r) * 24, 8), 16) for r in range(2)]
        return jnp.stack([total[a, :] for a in at])

    for r in range(2):
        tokf[pl.ds(r * 32, 32), :] = stage[pl.ds(pl.multiple_of((me * 2 + r) * PITCH, 8), 32), :]
    comm.reduce(chip_rows, send_rows, relay_in, relay_out, final_in, sums, csend, relay_sem, final_sem)
    for half in range(2):
        for r in range(2):
            at = pl.ds(r * 32 + half * 16, 16)
            tokf[at, :] = tokf[at, :] + sums[half, r]
    for r in range(2):
        row_of(rowx, r, tokf, r * 32, 32)
    out_ref[...] = rowx[...].astype(BF16)


def layer(ep, *args):
    dma = pltpu.SemaphoreType.DMA
    v = pltpu.VMEM
    local = [v(a.shape[1:] if a.shape[0] == 1 and a.ndim == 3 else a.shape, a.dtype) for a in args]
    local[4:6] = [v((96, 4096), BF16)]
    del local[12]
    local.insert(12, v((8, LANES), F32))
    local[-2:] = [pltpu.SMEM(a.shape, a.dtype) for a in args[-2:]]
    outs = (
        jax.ShapeDtypeStruct((2, 4096), BF16),
        jax.ShapeDtypeStruct(args[13].shape, F32),
        jax.ShapeDtypeStruct(args[11].shape, BF16),
        jax.ShapeDtypeStruct(args[12].shape, BF16),
    )
    results = pl.pallas_call(
        functools.partial(layer_kernel, ep, len(args), len(outs)),
        out_shape=outs,
        in_specs=[hbm()] * len(args),
        out_specs=(vmem(),) * len(outs),
        scratch_shapes=[
            *local,
            v((ep, 2, 32, LANES), BF16), v((ep, 2, 32, LANES), BF16), v((ep, 64, LANES), BF16),
            v((64 * PITCH, LANES), F32), v((8192, LANES), BF16), v((64, 1024), F32), v((64, 4096), BF16),
            v((256, LANES), F32), v((ep, 8, LANES), BF16), v((ep, 8, LANES), BF16), v((64, LANES), F32),
            v((96, LANES), F32), v((24, LANES), F32),
            v((256, LANES), F32), v((256, LANES), F32), v((LANES, LANES), F32), v((32, LANES), F32),
            v((64, LANES), F32), v((64, LANES), F32), v((2, 4096), F32), v((2, 1024), F32), v((64, LANES), F32),
            v((64, 512), BF16), v((64, LANES), F32), v((4, 64, 512), BF16), v((4, 64, 512), BF16),
            v((64 * 24, LANES), F32),
            v((ep, 2, 16, LANES), BF16), v((18, 2, 16, LANES), BF16), v((8, 2, 16, LANES), BF16),
            v((14, 2, 16, LANES), BF16), v((2, 2, 16, LANES), F32),
            dma((22,)), dma, dma((ep,)), dma, dma((ep,)), dma, dma((ep,)), dma((4,)), dma((4,)), dma, dma((ep,)),
            dma, dma((18,)), dma((14,)),
        ],
        compiler_params=pltpu.CompilerParams(
            collective_id=0, has_side_effects=True, vmem_limit_bytes=VMEM_LIMIT
        ),
        name="layer",
    )(*(pltpu.with_memory_space_constraint(a, pltpu.HBM) for a in args))
    return pl.pallas_call(
        flush_kernel,
        out_shape=outs,
        in_specs=[vmem()] * len(outs),
        out_specs=(hbm(),) * len(outs),
        scratch_shapes=[dma((len(outs),))],
        compiler_params=pltpu.CompilerParams(vmem_limit_bytes=1024 * 1024),
        name="flush",
    )(*results)


def flush_kernel(*refs):
    n = len(refs) // 2
    copies = [pltpu.make_async_copy(refs[i], refs[n + i], refs[-1].at[i]) for i in range(n)]
    for c in copies:
        c.start()
    for c in copies:
        c.wait()


def body(
    ep, tokens_in, mix_gain, w_gate_z, w_value, w_in_bc, w_step, step_bias, decay_log, skip_gain, conv_x_weight,
    conv_bc_weight, conv_x_state, conv_bc_state, ssm_state, inner_gain, out_weight, ffn_gain, expert_gate,
    expert_up, expert_down, routes, route_weight,
):
    out, new_state, new_x, new_bc = layer(
        ep, tokens_in, mix_gain.reshape(32, LANES), w_gate_z, w_value, w_in_bc.T, w_step.T,
        step_bias.reshape(1, 64), decay_log.reshape(1, 64), skip_gain.reshape(1, 64), conv_x_weight,
        conv_bc_weight, conv_x_state.transpose(1, 0, 2), conv_bc_state.transpose(1, 0, 2), ssm_state,
        inner_gain.reshape(32, LANES), out_weight, ffn_gain.reshape(32, LANES), expert_gate, expert_up,
        expert_down, routes, route_weight,
    )
    return out, new_state, new_x.transpose(1, 0, 2), new_bc.transpose(1, 0, 2)


def solution(mesh):
    ep = mesh.shape["ep"]
    cols, rep = P(None, "ep"), P()
    placed = (
        P(GRP_EP, None), rep, cols, cols, cols, rep, rep, rep, rep, rep, rep,
        P(GRP_EP, None, None), P(GRP_EP, None, None), P(GRP_EP, None, None, None),
        rep, cols, rep, P("ep", None, None), P("ep", None, None), P("ep", None, None),
        P(GRP_EP, None), P(GRP_EP, None),
    )
    return jax.shard_map(
        functools.partial(body, ep),
        mesh=mesh,
        in_specs=placed,
        out_specs=(
            P(GRP_EP, None),
            P(GRP_EP, None, None, None),
            P(GRP_EP, None, None),
            P(GRP_EP, None, None),
        ),
        check_vma=False,
    )
```
